512 devices in a mesh: sp: 64 (over z, y), tp: 8 (over x, core).
Axes of the slice: x: 4, y: 8, z: 8, core: 2. Of those that a mesh axis runs over, the one named last changes fastest.
Arguments:
- activations: bfloat16 [65536, 2048], P(('sp', 'tp')), may hold values from -6 to 6
- input_norm_scale: float32 [2048], replicated, may hold values from 0.1 to 1.9
- value_weight_matrix: bfloat16 [2048, 1024], P(None, 'tp'), may hold values from -0.125 to 0.125
- gate_weight_matrix: bfloat16 [2048, 1024], P(None, 'tp'), may hold values from -0.125 to 0.125
- write_weight_matrix: bfloat16 [2048, 1024], P(None, 'tp'), may hold values from -0.125 to 0.125
- read_weight_matrix: bfloat16 [2048, 1024], P(None, 'tp'), may hold values from -0.125 to 0.125
- step_weight_matrix: bfloat16 [2048, 16], replicated, may hold values from -0.125 to 0.125
- pooling_input_matrix: bfloat16 [2048, 1024], P(None, 'tp'), may hold values from -0.125 to 0.125
- value_filter_weight: float32 [4, 1024], P(None, 'tp'), may hold values from -3 to 3
- write_filter_weight: float32 [4, 1024], P(None, 'tp'), may hold values from -3 to 3
- read_filter_weight: float32 [4, 1024], P(None, 'tp'), may hold values from -3 to 3
- head_log_decay_rate: float32 [16], replicated, may hold values from -12 to 0, as said below
- step_bias_offset: float32 [16, 65536], P('tp', 'sp'), may hold values from -3 to 0, as said below
- position_log_decay: float32 [16, 65536], P('tp', 'sp'), may hold values from -2 to 0, as said below
- gated_norm_scale: float32 [1024], P('tp'), may hold values from 0.1 to 1.9
- pooling_group_matrix: bfloat16 [16, 64, 64], P('tp'), may hold values from -0.75 to 0.75
- pooling_channel_scale: float32 [1024], P('tp'), may hold values from 0.1 to 1.9
- state_output_matrix: bfloat16 [1024, 2048], P('tp'), may hold values from -0.125 to 0.125
- pooling_output_matrix: bfloat16 [1024, 2048], P('tp'), may hold values from -0.125 to 0.125
Outputs:
- mixed: bfloat16 [65536, 2048], P(('sp', 'tp'))
The draws below stay inside these ranges and needn't reach their ends.
Inputs may be any that keep to these rules, and one draw needn't show every extreme that they name: `head_log_decay_rate`: each head's logarithmic decay rate. `step_bias_offset`: constant over each block of 128 positions. `position_log_decay`: zero except at a few positions of the sequence.
All inputs are finite; a program needn't handle non-finite values.
Results may differ from the reference program's by a relative error of at most 0.017.
Values may be sent and summed in bfloat16 or wider, within the bound.
No kernel may reach another device: no remote copies, remote signals or barrier semaphores. Data moves between devices by JAX's collectives and lax.ppermute only.
A program may use at most 64 MiB of HBM per device.

```python
import jax
import jax.numpy as jnp
from jax import lax

D = 2048
HEADS = 16
HEAD_DIM = 64
GROUPS = 8
STATE = 128
CONV = 4
BLOCK = 128
POOL_GROUPS = 16
POOL_DIM = 64
TOKENS = 65536
N_TP = 8


def draw_head_log_decay_rate(key, part):
    ranking = jax.random.permutation(key, HEADS)
    slow_count = HEADS // 2
    spread = jax.random.uniform(jax.random.fold_in(key, 1), (HEADS,), jnp.float32)
    slow_log = jnp.log(1.0 / TOKENS) + spread * jnp.log(6.0)
    fast_log = jnp.log(0.06) + spread * (jnp.log(0.4) - jnp.log(0.06))
    return jnp.where(ranking < slow_count, slow_log, fast_log).astype(jnp.float32)


def draw_step_bias_offset(key, part):
    lowest = -3.0
    highest = -1.0
    levels = jax.random.uniform(key, (HEADS, TOKENS // BLOCK), jnp.float32, lowest, highest)
    return jnp.repeat(levels, BLOCK, axis=1)


def draw_position_log_decay(key, part):
    places = jax.random.randint(key, (4,), 0, TOKENS)
    depth = jnp.log(jax.random.uniform(jax.random.fold_in(key, 1), (HEADS, 4), jnp.float32, 0.5, 0.8))
    hits = (jnp.arange(TOKENS)[None, :] == places[:, None]).astype(jnp.float32)
    return jnp.dot(depth, hits, precision=lax.Precision.HIGHEST)


def level_of(rng, shape, pieces, least, largest):
    def one(axis_at, parts):
        heights = jax.random.uniform(jax.random.fold_in(jax.random.fold_in(rng, 6), axis_at), (parts,), jnp.float32, least / len(pieces), largest / len(pieces))
        return jnp.repeat(jnp.exp(heights), shape[axis_at] // parts).reshape((-1,) + (1,) * (len(shape) - axis_at - 1))

    gain = one(*pieces[0])
    for cut in pieces[1:]:
        gain = gain * one(*cut)
    return gain


def gaussian(stream_key, extent, width, most, pieces=(), held_as=jnp.bfloat16):
    result = width * jax.random.normal(stream_key, extent, jnp.float32)
    if pieces:
        result = result * level_of(stream_key, extent, pieces, -0.22, 0.18)
    return jnp.clip(result, -most, most).astype(held_as)


def setup_inputs(seed: int = 0) -> dict:
    streams_of = jax.random.split(jax.random.key(seed), 20)
    return {
        "activations": gaussian(streams_of[0], (TOKENS, D), 1.0, 6.0, ((0, 512),)),
        "input_norm_scale": jnp.clip(1.0 + 0.18 * jax.random.normal(streams_of[1], (D,), jnp.float32), 0.1, 1.9),
        "value_weight_matrix": gaussian(streams_of[2], (D, HEADS * HEAD_DIM), D ** -0.5, 0.125, ((1, 8),)),
        "gate_weight_matrix": gaussian(streams_of[3], (D, HEADS * HEAD_DIM), D ** -0.5, 0.125, ((1, 8),)),
        "write_weight_matrix": gaussian(streams_of[4], (D, GROUPS * STATE), D ** -0.5, 0.125, ((1, 8),)),
        "read_weight_matrix": gaussian(streams_of[5], (D, GROUPS * STATE), D ** -0.5, 0.125, ((1, 8),)),
        "step_weight_matrix": gaussian(streams_of[6], (D, HEADS), D ** -0.5, 0.125),
        "pooling_input_matrix": gaussian(streams_of[7], (D, POOL_GROUPS * POOL_DIM), D ** -0.5, 0.125, ((1, 8),)),
        "value_filter_weight": gaussian(streams_of[8], (CONV, HEADS * HEAD_DIM), CONV ** -0.5, 3.0, ((1, 8),), jnp.float32),
        "write_filter_weight": gaussian(streams_of[9], (CONV, GROUPS * STATE), CONV ** -0.5, 3.0, ((1, 8),), jnp.float32),
        "read_filter_weight": gaussian(streams_of[10], (CONV, GROUPS * STATE), CONV ** -0.5, 3.0, ((1, 8),), jnp.float32),
        "head_log_decay_rate": draw_head_log_decay_rate(jax.random.fold_in(streams_of[19], 71), 0),
        "step_bias_offset": draw_step_bias_offset(jax.random.fold_in(streams_of[19], 71), 0),
        "position_log_decay": draw_position_log_decay(jax.random.fold_in(streams_of[19], 71), 0),
        "gated_norm_scale": jnp.clip(1.0 + 0.18 * jax.random.normal(streams_of[14], (HEADS * HEAD_DIM,), jnp.float32), 0.1, 1.9),
        "pooling_group_matrix": gaussian(streams_of[15], (POOL_GROUPS, POOL_DIM, POOL_DIM), POOL_DIM ** -0.5, 0.75, ((0, 8),)),
        "pooling_channel_scale": jnp.clip(1.0 + 0.18 * jax.random.normal(streams_of[16], (POOL_GROUPS * POOL_DIM,), jnp.float32), 0.1, 1.9),
        "state_output_matrix": gaussian(streams_of[17], (HEADS * HEAD_DIM, D), (HEADS * HEAD_DIM + POOL_GROUPS * POOL_DIM) ** -0.5, 0.125, ((0, 8),)),
        "pooling_output_matrix": gaussian(streams_of[18], (POOL_GROUPS * POOL_DIM, D), (HEADS * HEAD_DIM + POOL_GROUPS * POOL_DIM) ** -0.5, 0.125, ((0, 8),)),
    }


EPS = 1e-06

def rounded(value):
    return lax.optimization_barrier(value.astype(jnp.bfloat16)).astype(jnp.float32)

def convolve(signal, taps):
    length = signal.shape[0]
    padded = jnp.pad(signal.astype(jnp.float32), ((taps.shape[0] - 1, 0), (0, 0)))
    summed = jnp.zeros(signal.shape, jnp.float32)
    for offset in range(taps.shape[0]):
        summed = summed + taps[offset] * padded[offset:offset + length]
    return jax.nn.silu(summed).astype(jnp.bfloat16)

def reference(activations, input_norm_scale, value_weight_matrix, gate_weight_matrix, write_weight_matrix, read_weight_matrix, step_weight_matrix, pooling_input_matrix, value_filter_weight, write_filter_weight, read_filter_weight, head_log_decay_rate, step_bias_offset, position_log_decay, gated_norm_scale, pooling_group_matrix, pooling_channel_scale, state_output_matrix, pooling_output_matrix):
    inputs_wide = activations.astype(jnp.float32)
    normed = (inputs_wide * lax.rsqrt(lax.optimization_barrier(jnp.mean(inputs_wide * inputs_wide, axis=-1, keepdims=True)) + EPS) * input_norm_scale).astype(jnp.bfloat16)
    value_in, gate_in, write_in, read_in, step_in, pool_in = [jnp.dot(normed, matrix, preferred_element_type=jnp.float32).astype(jnp.bfloat16) for matrix in (value_weight_matrix, gate_weight_matrix, write_weight_matrix, read_weight_matrix, step_weight_matrix, pooling_input_matrix)]
    values = convolve(value_in, value_filter_weight)
    writes = convolve(write_in, write_filter_weight)
    reads = convolve(read_in, read_filter_weight)
    step_length_value = jax.nn.softplus(step_in.astype(jnp.float32) + step_bias_offset.T)
    decay_logarithm_value = position_log_decay.T - jnp.exp(head_log_decay_rate) * step_length_value
    blocks = TOKENS // BLOCK
    repeat = HEADS // GROUPS
    values = values.reshape(blocks, BLOCK, HEADS, HEAD_DIM).astype(jnp.float32)
    writes = writes.reshape(blocks, BLOCK, GROUPS, STATE).astype(jnp.float32)
    reads = reads.reshape(blocks, BLOCK, GROUPS, STATE).astype(jnp.float32)
    cumulative = jnp.cumsum(decay_logarithm_value.reshape(blocks, BLOCK, HEADS), axis=1).transpose(0, 2, 1)
    step_heads = step_length_value.reshape(blocks, BLOCK, HEADS).transpose(0, 2, 1)
    causal = jnp.tril(jnp.ones((BLOCK, BLOCK), bool))
    affinity = jnp.repeat(jnp.einsum('btgn,bsgn->bgts', reads, writes), repeat, axis=1)
    spacing = cumulative[:, :, :, None] - cumulative[:, :, None, :]
    within = rounded(affinity * jnp.exp(jnp.where(causal, spacing, -jnp.inf)) * step_heads[:, :, None, :])
    inside = jnp.einsum('bhts,bshp->bthp', within, values)
    to_end = jnp.exp(cumulative[:, :, -1:] - cumulative) * step_heads
    weighted = rounded(values * to_end.transpose(0, 2, 1)[..., None])
    writes_heads = jnp.repeat(writes, repeat, axis=2)
    contrib = jnp.einsum('bshp,bshn->bhpn', weighted, writes_heads)
    totals = cumulative[:, :, -1]

    def advance(carried, block_pair):
        block_contrib, block_total = block_pair
        return (carried * jnp.exp(block_total)[:, None, None] + block_contrib, carried)
    _, entering = lax.scan(advance, jnp.zeros((HEADS, HEAD_DIM, STATE), jnp.float32), (contrib, totals))
    reads_heads = jnp.repeat(reads, repeat, axis=2)
    carried_in = jnp.einsum('bthn,bhpn->bthp', reads_heads, rounded(entering))
    state_y = inside + carried_in * jnp.exp(cumulative).transpose(0, 2, 1)[..., None]
    gated = state_y.reshape(TOKENS, HEADS * HEAD_DIM) * jax.nn.silu(gate_in.astype(jnp.float32))
    grouped = gated.reshape(TOKENS, GROUPS, repeat * HEAD_DIM)
    grouped = grouped * lax.rsqrt(lax.optimization_barrier(jnp.mean(grouped * grouped, axis=-1, keepdims=True)) + EPS)
    state_branch = (grouped.reshape(TOKENS, HEADS * HEAD_DIM) * gated_norm_scale).astype(jnp.bfloat16)
    pool_width = POOL_GROUPS * POOL_DIM
    pool_wide = pool_in.astype(jnp.float32)
    running = jnp.concatenate([jnp.zeros((1, pool_width), jnp.float32), jnp.cumsum(pool_wide, axis=0)], axis=0)
    level = jnp.arange(pool_width, dtype=jnp.int32) // POOL_DIM % 4
    window_len = jnp.power(2, level + 1).astype(jnp.int32)[None, :]
    position = jnp.arange(TOKENS, dtype=jnp.int32)[:, None]
    lowest = jnp.maximum(position + 1 - window_len, 0).astype(jnp.int32)
    lower_sum = jnp.take_along_axis(running, lowest, axis=0)
    counted = jnp.minimum(position + 1, window_len).astype(jnp.float32)
    pool_diff = rounded((running[1:] - lower_sum) / counted - pool_wide)
    pooled = jnp.einsum('tgc,gcd->tgd', pool_diff.reshape(TOKENS, POOL_GROUPS, POOL_DIM), pooling_group_matrix.astype(jnp.float32))
    pool_branch = (pooled.reshape(TOKENS, pool_width) * pooling_channel_scale).astype(jnp.bfloat16)
    head_cols = HEADS * HEAD_DIM // N_TP
    pool_cols = pool_width // N_TP
    summed = jnp.zeros((TOKENS, D), jnp.float32)
    for member in range(N_TP):
        part_sum = jnp.dot(state_branch[:, member * head_cols:(member + 1) * head_cols], state_output_matrix[member * head_cols:(member + 1) * head_cols], preferred_element_type=jnp.float32) + jnp.dot(pool_branch[:, member * pool_cols:(member + 1) * pool_cols], pooling_output_matrix[member * pool_cols:(member + 1) * pool_cols], preferred_element_type=jnp.float32)
        summed = summed + rounded(part_sum)
    return summed.astype(jnp.bfloat16)
```

```python
import jax
import jax.numpy as jnp
from jax import lax
from jax.experimental import pallas as pl
from jax.experimental.pallas import tpu as pltpu
from jax.sharding import Mesh
from jax.sharding import PartitionSpec as P

HEAD_DIM = 64
STATE = 128
BLOCK = 128
POOL_DIM = 64
HALO = 16
SP = ("sp_0", "sp_1")
SP_TP = ("sp_0", "sp_1", "tp")
EPS = 1e-06
F32 = jnp.float32
BF16 = jnp.bfloat16
STEP_ROWS = 256
PACKED = STATE + 16


def silu(x):
    return x / (1.0 + jnp.exp(-x))


def by_head(first, second, shape):
    lane = lax.broadcasted_iota(jnp.int32, shape, len(shape) - 1)
    return jnp.where(lane < HEAD_DIM, first, second)


def mix_kernel(
    base_ref,
    x_ref,
    w_ref,
    halo_ref,
    taps_ref,
    bias_ref,
    pld_ref,
    rate_ref,
    pool_row_ref,
    pool_matrix_ref,
    y_ref,
    reads_ref,
    reach_ref,
    gate_ref,
    pool_ref,
    state_ref,
    conv_tail,
    pool_tail,
    carried_ref,
    prefix_ref,
):
    turn = pl.program_id(0)
    rows = x_ref.shape[0]

    @pl.when(turn == 0)
    def _():
        conv_tail[...] = halo_ref[:, : 3 * STATE].astype(F32)
        pool_tail[...] = halo_ref[:, 3 * STATE :].astype(F32)
        carried_ref[...] = jnp.zeros_like(carried_ref)
        prefix_ref[...] = jnp.zeros_like(prefix_ref)

    projected = jnp.dot(x_ref[...], w_ref[...], preferred_element_type=F32).astype(BF16)
    conv_in = projected[:, : 3 * STATE].astype(F32)
    pool_in = projected[:, 3 * STATE : 4 * STATE].astype(F32)
    gate_ref[...] = silu(projected[:, 4 * STATE : 5 * STATE].astype(F32))
    step_in = projected[:, 5 * STATE :].astype(F32)

    extended = jnp.concatenate([conv_tail[...], conv_in], axis=0)
    conv_tail[...] = conv_in[rows - HALO :]
    summed = extended * taps_ref[3:4, :]
    for back in range(1, 4):
        summed = summed + pltpu.roll(extended, back, 0) * taps_ref[3 - back : 4 - back, :]
    convolved = silu(summed[HALO:]).astype(BF16)

    wide = jnp.concatenate([pool_tail[...], pool_in], axis=0)
    pool_tail[...] = pool_in[rows - HALO :]
    sum_two = wide + pltpu.roll(wide, 1, 0)
    sum_four = sum_two + pltpu.roll(sum_two, 2, 0)
    sum_eight = sum_four + pltpu.roll(sum_four, 4, 0)
    sum_sixteen = sum_eight + pltpu.roll(sum_eight, 8, 0)
    window = pool_row_ref[0:1, :]
    window_sum = jnp.where(
        window == 2.0,
        sum_two,
        jnp.where(window == 4.0, sum_four, jnp.where(window == 8.0, sum_eight, sum_sixteen)),
    )[HALO:]
    position = (
        base_ref[0] + turn * rows + lax.broadcasted_iota(jnp.int32, (rows, 1), 0) + 1
    ).astype(F32)
    difference = (window_sum / jnp.minimum(position, window) - pool_in).astype(BF16)
    pooled = jnp.dot(difference, pool_matrix_ref[...], preferred_element_type=F32)
    pool_ref[...] = (pooled * pool_row_ref[1:2, :]).astype(BF16)

    square = (BLOCK, BLOCK)
    row_at = lax.broadcasted_iota(jnp.int32, square, 0)
    col_at = lax.broadcasted_iota(jnp.int32, square, 1)
    upper = (row_at <= col_at).astype(F32)
    causal = row_at >= col_at
    carried = carried_ref[...]
    prefix = prefix_ref[0:2, :]
    for k in range(rows // BLOCK):
        at = slice(k * BLOCK, (k + 1) * BLOCK)
        values = convolved[at, :STATE]
        writes = convolved[at, STATE : 2 * STATE]
        reads = convolved[at, 2 * STATE :]
        step = jax.nn.softplus(step_in[at].T[0:2, :] + bias_ref[:, at])
        log_decay = pld_ref[:, at] - rate_ref[...] * step
        cum = jnp.dot(
            jnp.concatenate([log_decay, jnp.zeros((6, BLOCK), F32)], axis=0),
            upper,
            precision=lax.Precision.HIGHEST,
            preferred_element_type=F32,
        )[0:2]
        total = cum[:, BLOCK - 1 :]
        to_end = jnp.exp(total - cum) * step
        columns = jnp.concatenate(
            [cum, to_end, jnp.exp(cum), jnp.exp(prefix + cum)], axis=0
        ).T
        affinity = lax.dot_general(
            reads, writes, (((1,), (1,)), ((), ())), preferred_element_type=F32
        )
        inside = []
        for h in range(2):
            spacing = columns[:, h : h + 1] - cum[h : h + 1, :]
            within = affinity * jnp.exp(jnp.where(causal, spacing, -jnp.inf)) * step[h : h + 1, :]
            inside.append(jnp.dot(within.astype(BF16), values, preferred_element_type=F32))
        weighted = (
            values.astype(F32) * by_head(columns[:, 2:3], columns[:, 3:4], square)
        ).astype(BF16)
        contrib = lax.dot_general(
            writes, weighted, (((0,), (0,)), ((), ())), preferred_element_type=F32
        )
        local = jnp.dot(reads, carried.astype(BF16), preferred_element_type=F32)
        y_ref[at, :] = by_head(inside[0], inside[1], square) + local * by_head(
            columns[:, 4:5], columns[:, 5:6], square
        )
        reach_ref[at, :] = by_head(columns[:, 6:7], columns[:, 7:8], square)
        reads_ref[at, :] = reads
        decay = by_head(total[0:1, :], total[1:2, :], (1, STATE))
        carried = carried * jnp.exp(decay) + contrib
        prefix = prefix + total
    carried_ref[...] = carried
    prefix_ref[0:2, :] = prefix

    @pl.when(turn == pl.num_programs(0) - 1)
    def _():
        packed = pack(carried, by_head(prefix[0:1, :], prefix[1:2, :], (1, STATE)))
        for k in range(state_ref.shape[0]):
            state_ref[k] = packed


def pack(state, total):
    high = total.astype(BF16)
    low = (total - high.astype(F32)).astype(BF16)
    row = lax.broadcasted_iota(jnp.int32, (PACKED - STATE, STATE), 0)
    tail = jnp.where(row == 0, high.astype(F32), jnp.where(row == 1, low.astype(F32), 0.0))
    return jnp.concatenate([state.astype(BF16), tail.astype(BF16)], axis=0)


def scan_pieces(pieces_ref, here):
    state = before_state = jnp.zeros((STATE, STATE), F32)
    total = before_total = jnp.zeros((1, STATE), F32)
    for k in range(pieces_ref.shape[0]):
        tail = pieces_ref[k, STATE:, :].astype(F32)
        decay = tail[0:1, :] + tail[1:2, :]
        state = state * jnp.exp(decay) + pieces_ref[k, :STATE, :].astype(F32)
        total = total + decay
        passed = k < here
        before_state = jnp.where(passed, state, before_state)
        before_total = jnp.where(passed, total, before_total)
    return state, total, before_state, before_total


def row_scan_kernel(here_ref, pieces_ref, before_ref, packed_ref):
    state, total, before_state, before_total = scan_pieces(pieces_ref, here_ref[0])
    before_ref[:STATE, :] = before_state
    before_ref[STATE:, :] = jnp.broadcast_to(before_total, (8, STATE))
    packed = pack(state, total)
    for k in range(packed_ref.shape[0]):
        packed_ref[k] = packed


def finish_kernel(
    here_ref,
    pieces_ref,
    before_ref,
    y_ref,
    reads_ref,
    reach_ref,
    gate_ref,
    pool_ref,
    scale_ref,
    out_ref,
):
    _, _, rows_before, _ = scan_pieces(pieces_ref, here_ref[0])
    incoming = rows_before * jnp.exp(before_ref[STATE : STATE + 1, :]) + before_ref[:STATE, :]
    crossed = jnp.dot(reads_ref[...], incoming.astype(BF16), preferred_element_type=F32)
    gated = (y_ref[...] + crossed * reach_ref[...]) * gate_ref[...]
    norm = lax.rsqrt(jnp.mean(gated * gated, axis=-1, keepdims=True) + EPS)
    out_ref[:, :STATE] = (gated * norm * scale_ref[...]).astype(BF16)
    out_ref[:, STATE:] = pool_ref[...]


def output_kernel(rows_ref, w_ref, out_ref):
    total = jnp.zeros(out_ref.shape, F32)
    for k in range(rows_ref.shape[0]):
        total = total + jnp.dot(rows_ref[k], w_ref[k], preferred_element_type=F32)
    out_ref[...] = total.astype(BF16)


def whole(shape):
    return pl.BlockSpec(shape, lambda *_: (0,) * len(shape))


def normalize(rows, scale):
    wide = rows.astype(F32)
    return (wide * lax.rsqrt(jnp.mean(wide * wide, axis=-1, keepdims=True) + EPS) * scale).astype(
        BF16
    )


def rows_before(rows, members):
    ranges = lax.axis_size(SP)
    route = [(i * members + members - 1, (i + 1) * members) for i in range(ranges - 1)]
    found = lax.ppermute(rows, SP_TP, route)
    reach = 1
    while reach < members:
        sends = [(i, i + reach) for i in range(reach) if i + reach < members]
        found = found + lax.ppermute(found, "tp", sends)
        reach *= 2
    return found


def shards(
    activations,
    input_norm_scale,
    value_weight_matrix,
    gate_weight_matrix,
    write_weight_matrix,
    read_weight_matrix,
    step_weight_matrix,
    pooling_input_matrix,
    value_filter_weight,
    write_filter_weight,
    read_filter_weight,
    head_log_decay_rate,
    step_bias_offset,
    position_log_decay,
    gated_norm_scale,
    pooling_group_matrix,
    pooling_channel_scale,
    state_output_matrix,
    pooling_output_matrix,
):
    tp_rank = lax.axis_index("tp")
    sp_rank = lax.axis_index(SP)
    members = lax.axis_size("tp")
    own_rows, width = activations.shape
    length = own_rows * members
    heads = step_bias_offset.shape[0]

    normed = normalize(activations, input_norm_scale)
    shard_rows = lax.all_gather(normed, "tp", axis=0, tiled=True)

    halo_rows = normalize(rows_before(activations[own_rows - HALO :], members), input_norm_scale)
    step_weights = lax.dynamic_slice_in_dim(step_weight_matrix, tp_rank * heads, heads, 1)
    weights = jnp.concatenate(
        [
            value_weight_matrix,
            write_weight_matrix,
            read_weight_matrix,
            pooling_input_matrix,
            gate_weight_matrix,
            jnp.pad(step_weights, ((0, 0), (0, STATE - heads))),
        ],
        axis=1,
    )
    halo = jnp.dot(halo_rows, weights[:, : 4 * STATE], preferred_element_type=F32).astype(BF16)
    taps = jnp.concatenate([value_filter_weight, write_filter_weight, read_filter_weight], axis=1)
    taps = jnp.pad(taps, ((0, 4), (0, 0)))
    rates = jnp.exp(lax.dynamic_slice_in_dim(head_log_decay_rate, tp_rank * heads, heads, 0))
    rates = jnp.broadcast_to(rates[:, None], (heads, BLOCK))
    pool_groups = pooling_group_matrix.shape[0]
    level = (tp_rank * pool_groups + jnp.arange(pool_groups, dtype=jnp.int32)) % 4
    window = jnp.repeat(jnp.left_shift(2, level).astype(F32), POOL_DIM)
    pool_rows = jnp.pad(jnp.stack([window, pooling_channel_scale]), ((0, 6), (0, 0)))
    empty = jnp.zeros((POOL_DIM, POOL_DIM), BF16)
    pool_matrix = jnp.block(
        [[pooling_group_matrix[0], empty], [empty, pooling_group_matrix[1]]]
    )
    base = (sp_rank * length).astype(jnp.int32).reshape(1)

    own_output = jnp.concatenate([state_output_matrix, pooling_output_matrix], axis=0)
    shard_rows, own_output, halo, weights, taps, rates, pool_rows, pool_matrix = (
        lax.optimization_barrier(
            (shard_rows, own_output, halo, weights, taps, rates, pool_rows, pool_matrix)
        )
    )
    output_weights = lax.all_gather(own_output, "tp", axis=0)

    steps = length // STEP_ROWS
    ring = lax.axis_size("sp_1")
    columns = lax.axis_size("sp_0")
    by_rows = lambda cols: pl.BlockSpec((STEP_ROWS, cols), lambda i: (i, 0))
    y, reads, reach, gate, pool, packed = pl.pallas_call(
        mix_kernel,
        name="mix",
        grid=(steps,),
        in_specs=[
            pl.BlockSpec(memory_space=pltpu.SMEM),
            by_rows(width),
            whole(weights.shape),
            whole(halo.shape),
            whole(taps.shape),
            pl.BlockSpec((heads, STEP_ROWS), lambda i: (0, i)),
            pl.BlockSpec((heads, STEP_ROWS), lambda i: (0, i)),
            whole(rates.shape),
            whole(pool_rows.shape),
            whole(pool_matrix.shape),
        ],
        out_specs=[by_rows(STATE)] * 5 + [whole((ring, PACKED, STATE))],
        out_shape=[
            jax.ShapeDtypeStruct((length, STATE), F32),
            jax.ShapeDtypeStruct((length, STATE), BF16),
            jax.ShapeDtypeStruct((length, STATE), F32),
            jax.ShapeDtypeStruct((length, STATE), F32),
            jax.ShapeDtypeStruct((length, STATE), BF16),
            jax.ShapeDtypeStruct((ring, PACKED, STATE), BF16),
        ],
        scratch_shapes=[
            pltpu.VMEM((HALO, 3 * STATE), F32),
            pltpu.VMEM((HALO, STATE), F32),
            pltpu.VMEM((STATE, STATE), F32),
            pltpu.VMEM((8, STATE), F32),
        ],
        compiler_params=pltpu.CompilerParams(dimension_semantics=("arbitrary",)),
    )(
        base,
        shard_rows,
        weights,
        halo,
        taps,
        step_bias_offset,
        position_log_decay,
        rates,
        pool_rows,
        pool_matrix,
    )

    pieces = lax.all_to_all(packed, "sp_1", 0, 0, tiled=True)
    before, packed = pl.pallas_call(
        row_scan_kernel,
        name="row_scan",
        in_specs=[pl.BlockSpec(memory_space=pltpu.SMEM), whole(pieces.shape)],
        out_specs=[whole((STATE + 8, STATE)), whole((columns, PACKED, STATE))],
        out_shape=[
            jax.ShapeDtypeStruct((STATE + 8, STATE), F32),
            jax.ShapeDtypeStruct((columns, PACKED, STATE), BF16),
        ],
        grid=(1,),
    )(lax.axis_index("sp_1").astype(jnp.int32).reshape(1), pieces)
    pieces = lax.all_to_all(packed, "sp_0", 0, 0, tiled=True)
    branches = pl.pallas_call(
        finish_kernel,
        name="finish",
        in_specs=[
            pl.BlockSpec(memory_space=pltpu.SMEM),
            whole(pieces.shape),
            whole(before.shape),
            whole(y.shape),
            whole(reads.shape),
            whole(reach.shape),
            whole(gate.shape),
            whole(pool.shape),
            whole((1, STATE)),
        ],
        out_specs=whole((length, 2 * STATE)),
        out_shape=jax.ShapeDtypeStruct((length, 2 * STATE), BF16),
        grid=(1,),
    )(
        lax.axis_index("sp_0").astype(jnp.int32).reshape(1),
        pieces,
        before,
        y,
        reads,
        reach,
        gate,
        pool,
        gated_norm_scale.reshape(1, STATE),
    )
    branches = lax.all_to_all(
        branches.reshape(members, own_rows, 2 * STATE), "tp", 0, 0, tiled=True
    )
    tile = 256
    return pl.pallas_call(
        output_kernel,
        name="output",
        in_specs=[
            whole(branches.shape),
            pl.BlockSpec((members, 2 * STATE, tile), lambda i: (0, 0, i)),
        ],
        out_specs=pl.BlockSpec((own_rows, tile), lambda i: (0, i)),
        out_shape=jax.ShapeDtypeStruct((own_rows, width), BF16),
        grid=(width // tile,),
    )(branches, output_weights)


def solution(mesh):
    ranges = mesh.shape["sp"]
    inner = 8 if ranges % 8 == 0 else 2
    torus = Mesh(mesh.devices.reshape(ranges // inner, inner, mesh.shape["tp"]), SP_TP)
    in_specs = (
        P(SP_TP, None),
        P(),
        P(None, "tp"),
        P(None, "tp"),
        P(None, "tp"),
        P(None, "tp"),
        P(),
        P(None, "tp"),
        P(None, "tp"),
        P(None, "tp"),
        P(None, "tp"),
        P(),
        P("tp", SP),
        P("tp", SP),
        P("tp"),
        P("tp", None, None),
        P("tp"),
        P("tp", None),
        P("tp", None),
    )
    return jax.shard_map(
        shards, mesh=torus, in_specs=in_specs, out_specs=P(SP_TP, None), check_vma=False
    )
```

```python
import jax
import jax.numpy as jnp
from jax import lax
from jax.experimental import pallas as pl
from jax.experimental.pallas import tpu as pltpu
from jax.sharding import Mesh
from jax.sharding import PartitionSpec as P

HEAD_DIM = 64
STATE = 128
BLOCK = 128
POOL_DIM = 64
HALO = 16
SP = ("sp_0", "sp_1")
SP_TP = ("sp_0", "sp_1", "tp")
EPS = 1e-06
F32 = jnp.float32
BF16 = jnp.bfloat16
STEP_ROWS = 256
PACKED = STATE + 16


def silu(x):
    return x / (1.0 + jnp.exp(-x))


def by_head(first, second, shape):
    lane = lax.broadcasted_iota(jnp.int32, shape, len(shape) - 1)
    return jnp.where(lane < HEAD_DIM, first, second)


def mix_kernel(
    base_ref,
    rows_ref,
    w_ref,
    halo_ref,
    taps_ref,
    lanes_ref,
    pool_matrix_ref,
    y_ref,
    reads_ref,
    reach_ref,
    gate_ref,
    pool_ref,
    state_ref,
    x_ref,
    conv_in,
    pool_in,
    step_in,
    mixed_ref,
    arrived,
):
    length = rows_ref.shape[0]
    chunks = length // STEP_ROWS
    blocks = length // BLOCK
    pairs = 2 * blocks
    bias, pld, rate = (lanes_ref[k * pairs : (k + 1) * pairs] for k in range(3))
    window = lanes_ref[3 * pairs : 3 * pairs + 1]
    pool_scale = lanes_ref[3 * pairs + 1 : 3 * pairs + 2]
    incoming = [
        pltpu.make_async_copy(
            rows_ref.at[pl.ds(c * STEP_ROWS, STEP_ROWS)], x_ref.at[c], arrived.at[c]
        )
        for c in range(chunks)
    ]
    for copy in incoming:
        copy.start()
    conv_in[:HALO] = halo_ref[:, : 3 * STATE].astype(F32)
    pool_in[:HALO] = halo_ref[:, 3 * STATE :].astype(F32)
    for c in range(chunks):
        first = c * STEP_ROWS
        at = slice(first, first + STEP_ROWS)
        shifted = slice(HALO + first, HALO + first + STEP_ROWS)
        reached = slice(first, first + HALO + STEP_ROWS)
        incoming[c].wait()
        projected = jnp.dot(x_ref[c], w_ref[...], preferred_element_type=F32).astype(BF16)
        conv_in[shifted] = projected[:, : 3 * STATE].astype(F32)
        pool_in[shifted] = projected[:, 3 * STATE : 4 * STATE].astype(F32)
        gate_ref[at] = silu(projected[:, 4 * STATE : 5 * STATE].astype(F32))
        step_in[at] = projected[:, 5 * STATE :].astype(F32)

        extended = conv_in[reached]
        summed = extended * taps_ref[3:4, :]
        for back in range(1, 4):
            summed = summed + pltpu.roll(extended, back, 0) * taps_ref[3 - back : 4 - back, :]
        convolved = silu(summed[HALO:]).astype(BF16)
        mixed_ref[at] = convolved[:, : 2 * STATE]
        reads_ref[at] = convolved[:, 2 * STATE :]

        wide = pool_in[reached]
        sum_two = wide + pltpu.roll(wide, 1, 0)
        sum_four = sum_two + pltpu.roll(sum_two, 2, 0)
        sum_eight = sum_four + pltpu.roll(sum_four, 4, 0)
        sum_sixteen = sum_eight + pltpu.roll(sum_eight, 8, 0)
        window_sum = jnp.where(
            window == 2.0,
            sum_two,
            jnp.where(window == 4.0, sum_four, jnp.where(window == 8.0, sum_eight, sum_sixteen)),
        )[HALO:]
        position = (
            base_ref[0] + first + 1 + lax.broadcasted_iota(jnp.int32, (STEP_ROWS, 1), 0)
        ).astype(F32)
        difference = (window_sum / jnp.minimum(position, window) - wide[HALO:]).astype(BF16)
        pooled = jnp.dot(difference, pool_matrix_ref[...], preferred_element_type=F32)
        pool_ref[at] = (pooled * pool_scale).astype(BF16)

    square = (BLOCK, BLOCK)
    row_at = lax.broadcasted_iota(jnp.int32, square, 0)
    col_at = lax.broadcasted_iota(jnp.int32, square, 1)
    upper = (row_at <= col_at).astype(F32)
    causal = row_at >= col_at
    spread = step_in[:BLOCK]
    for b in range(1, blocks):
        spread = spread + pltpu.roll(step_in[b * BLOCK : (b + 1) * BLOCK], 2 * b, 1)
    step = jax.nn.softplus(spread.T[:pairs] + bias)
    cum = jnp.dot(
        pld - rate * step,
        upper,
        precision=lax.Precision.HIGHEST,
        preferred_element_type=F32,
    )
    total = jnp.broadcast_to(cum[:, BLOCK - 1 :], (pairs, BLOCK))
    prefix = jnp.zeros((2, BLOCK), F32)
    prefixes = []
    for b in range(blocks):
        prefixes.append(prefix)
        prefix = prefix + total[2 * b : 2 * b + 2]
    columns = jnp.concatenate(
        [
            cum,
            jnp.exp(total - cum) * step,
            jnp.exp(cum),
            jnp.exp(jnp.concatenate(prefixes, axis=0) + cum),
            jnp.zeros((BLOCK - 4 * pairs, BLOCK), F32),
        ],
        axis=0,
    ).T

    def column(kind, b, h):
        j = kind * pairs + 2 * b + h
        return columns[:, j : j + 1]

    carried = jnp.zeros((STATE, STATE), F32)
    for b in range(blocks):
        at = slice(b * BLOCK, (b + 1) * BLOCK)
        values = mixed_ref[at, :STATE]
        writes = mixed_ref[at, STATE:]
        reads = reads_ref[at]
        affinity = lax.dot_general(
            reads, writes, (((1,), (1,)), ((), ())), preferred_element_type=F32
        )
        inside = []
        for h in range(2):
            row = 2 * b + h
            spacing = column(0, b, h) - cum[row : row + 1]
            within = affinity * jnp.exp(jnp.where(causal, spacing, -jnp.inf)) * step[row : row + 1]
            inside.append(jnp.dot(within.astype(BF16), values, preferred_element_type=F32))
        weighted = (
            values.astype(F32) * by_head(column(1, b, 0), column(1, b, 1), square)
        ).astype(BF16)
        contrib = lax.dot_general(
            writes, weighted, (((0,), (0,)), ((), ())), preferred_element_type=F32
        )
        local = jnp.dot(reads, carried.astype(BF16), preferred_element_type=F32)
        y_ref[at] = by_head(inside[0], inside[1], square) + local * by_head(
            column(2, b, 0), column(2, b, 1), square
        )
        reach_ref[at] = by_head(column(3, b, 0), column(3, b, 1), square)
        decay = by_head(total[2 * b : 2 * b + 1], total[2 * b + 1 : 2 * b + 2], (1, STATE))
        carried = carried * jnp.exp(decay) + contrib
    packed = pack(carried, by_head(prefix[0:1], prefix[1:2], (1, STATE)))
    for k in range(state_ref.shape[0]):
        state_ref[k] = packed


def pack(state, total):
    high = total.astype(BF16)
    low = (total - high.astype(F32)).astype(BF16)
    row = lax.broadcasted_iota(jnp.int32, (PACKED - STATE, STATE), 0)
    tail = jnp.where(row == 0, high.astype(F32), jnp.where(row == 1, low.astype(F32), 0.0))
    return jnp.concatenate([state.astype(BF16), tail.astype(BF16)], axis=0)


def scan_pieces(pieces_ref, here):
    state = before_state = jnp.zeros((STATE, STATE), F32)
    total = before_total = jnp.zeros((1, STATE), F32)
    for k in range(pieces_ref.shape[0]):
        tail = pieces_ref[k, STATE:, :].astype(F32)
        decay = tail[0:1, :] + tail[1:2, :]
        state = state * jnp.exp(decay) + pieces_ref[k, :STATE, :].astype(F32)
        total = total + decay
        passed = k < here
        before_state = jnp.where(passed, state, before_state)
        before_total = jnp.where(passed, total, before_total)
    return state, total, before_state, before_total


def row_scan_kernel(here_ref, pieces_ref, before_ref, packed_ref):
    state, total, before_state, before_total = scan_pieces(pieces_ref, here_ref[0])
    before_ref[:STATE, :] = before_state
    before_ref[STATE:, :] = jnp.broadcast_to(before_total, (8, STATE))
    packed = pack(state, total)
    for k in range(packed_ref.shape[0]):
        packed_ref[k] = packed


def finish_kernel(
    here_ref,
    pieces_ref,
    before_ref,
    y_ref,
    reads_ref,
    reach_ref,
    gate_ref,
    pool_ref,
    scale_ref,
    out_ref,
):
    _, _, rows_before, _ = scan_pieces(pieces_ref, here_ref[0])
    incoming = rows_before * jnp.exp(before_ref[STATE : STATE + 1, :]) + before_ref[:STATE, :]
    crossed = jnp.dot(reads_ref[...], incoming.astype(BF16), preferred_element_type=F32)
    gated = (y_ref[...] + crossed * reach_ref[...]) * gate_ref[...]
    norm = lax.rsqrt(jnp.mean(gated * gated, axis=-1, keepdims=True) + EPS)
    out_ref[:, :STATE] = (gated * norm * scale_ref[...]).astype(BF16)
    out_ref[:, STATE:] = pool_ref[...]


def output_kernel(rows_ref, w_ref, out_ref, weights_ref, arrived):
    parts = rows_ref.shape[0]
    incoming = [
        pltpu.make_async_copy(w_ref.at[k], weights_ref.at[k], arrived.at[k]) for k in range(parts)
    ]
    for copy in incoming:
        copy.start()
    total = None
    for k in range(parts):
        incoming[k].wait()
        part = jnp.dot(rows_ref[k], weights_ref[k], preferred_element_type=F32)
        total = part if total is None else total + part
    out_ref[...] = total.astype(BF16)


def limits(mebibytes):
    return pltpu.CompilerParams(vmem_limit_bytes=mebibytes * 2**20)


def in_hbm(array):
    return pltpu.with_memory_space_constraint(array, pltpu.HBM)


def whole(shape):
    return pl.BlockSpec(shape, lambda *_: (0,) * len(shape))


def normalize(rows, scale):
    wide = rows.astype(F32)
    return (wide * lax.rsqrt(jnp.mean(wide * wide, axis=-1, keepdims=True) + EPS) * scale).astype(
        BF16
    )


def rows_before(rows, members):
    ranges = lax.axis_size(SP)
    route = [(i * members + members - 1, (i + 1) * members) for i in range(ranges - 1)]
    found = lax.ppermute(rows, SP_TP, route)
    reach = 1
    while reach < members:
        sends = [(i, i + reach) for i in range(reach) if i + reach < members]
        found = found + lax.ppermute(found, "tp", sends)
        reach *= 2
    return found


def shards(
    activations,
    input_norm_scale,
    value_weight_matrix,
    gate_weight_matrix,
    write_weight_matrix,
    read_weight_matrix,
    step_weight_matrix,
    pooling_input_matrix,
    value_filter_weight,
    write_filter_weight,
    read_filter_weight,
    head_log_decay_rate,
    step_bias_offset,
    position_log_decay,
    gated_norm_scale,
    pooling_group_matrix,
    pooling_channel_scale,
    state_output_matrix,
    pooling_output_matrix,
):
    tp_rank = lax.axis_index("tp")
    sp_rank = lax.axis_index(SP)
    members = lax.axis_size("tp")
    own_rows, width = activations.shape
    length = own_rows * members
    heads = step_bias_offset.shape[0]

    normed = normalize(activations, input_norm_scale)
    shard_rows = lax.all_gather(normed, "tp", axis=0, tiled=True)

    halo_rows = normalize(rows_before(activations[own_rows - HALO :], members), input_norm_scale)
    step_weights = lax.dynamic_slice_in_dim(step_weight_matrix, tp_rank * heads, heads, 1)
    weights = jnp.concatenate(
        [
            value_weight_matrix,
            write_weight_matrix,
            read_weight_matrix,
            pooling_input_matrix,
            gate_weight_matrix,
            jnp.pad(step_weights, ((0, 0), (0, STATE - heads))),
        ],
        axis=1,
    )
    halo = jnp.dot(halo_rows, weights[:, : 4 * STATE], preferred_element_type=F32).astype(BF16)
    taps = jnp.concatenate([value_filter_weight, write_filter_weight, read_filter_weight], axis=1)
    taps = jnp.pad(taps, ((0, 4), (0, 0)))
    rates = jnp.exp(lax.dynamic_slice_in_dim(head_log_decay_rate, tp_rank * heads, heads, 0))
    blocks = length // BLOCK
    rates = jnp.broadcast_to(jnp.tile(rates, blocks)[:, None], (heads * blocks, BLOCK))
    bias, pld = (
        lane_rows.reshape(heads, blocks, BLOCK).transpose(1, 0, 2).reshape(heads * blocks, BLOCK)
        for lane_rows in (step_bias_offset, position_log_decay)
    )
    pool_groups = pooling_group_matrix.shape[0]
    level = (tp_rank * pool_groups + jnp.arange(pool_groups, dtype=jnp.int32)) % 4
    window = jnp.repeat(jnp.left_shift(2, level).astype(F32), POOL_DIM)
    pool_rows = jnp.pad(jnp.stack([window, pooling_channel_scale]), ((0, 6), (0, 0)))
    empty = jnp.zeros((POOL_DIM, POOL_DIM), BF16)
    pool_matrix = jnp.block(
        [[pooling_group_matrix[0], empty], [empty, pooling_group_matrix[1]]]
    )
    base = (sp_rank * length).astype(jnp.int32).reshape(1)

    own_output = jnp.concatenate([state_output_matrix, pooling_output_matrix], axis=0)
    lanes = jnp.concatenate([bias, pld, rates, pool_rows], axis=0)
    shard_rows, own_output, halo, weights, taps, lanes, pool_matrix = lax.optimization_barrier(
        (shard_rows, own_output, halo, weights, taps, lanes, pool_matrix)
    )
    output_weights = lax.all_gather(own_output, "tp", axis=0)

    ring = lax.axis_size("sp_1")
    columns = lax.axis_size("sp_0")
    y, reads, reach, gate, pool, packed = pl.pallas_call(
        mix_kernel,
        name="mix",
        grid=(1,),
        in_specs=[
            pl.BlockSpec(memory_space=pltpu.SMEM),
            pl.BlockSpec(memory_space=pltpu.HBM),
            whole(weights.shape),
            whole(halo.shape),
            whole(taps.shape),
            whole(lanes.shape),
            whole(pool_matrix.shape),
        ],
        out_specs=[whole((length, STATE))] * 5 + [whole((ring, PACKED, STATE))],
        out_shape=[
            jax.ShapeDtypeStruct((length, STATE), F32),
            jax.ShapeDtypeStruct((length, STATE), BF16),
            jax.ShapeDtypeStruct((length, STATE), F32),
            jax.ShapeDtypeStruct((length, STATE), F32),
            jax.ShapeDtypeStruct((length, STATE), BF16),
            jax.ShapeDtypeStruct((ring, PACKED, STATE), BF16),
        ],
        scratch_shapes=[
            pltpu.VMEM((length // STEP_ROWS, STEP_ROWS, width), BF16),
            pltpu.VMEM((HALO + length, 3 * STATE), F32),
            pltpu.VMEM((HALO + length, STATE), F32),
            pltpu.VMEM((length, STATE), F32),
            pltpu.VMEM((length, 2 * STATE), BF16),
            pltpu.SemaphoreType.DMA((length // STEP_ROWS,)),
        ],
        compiler_params=limits(32),
    )(base, in_hbm(shard_rows), weights, halo, taps, lanes, pool_matrix)

    pieces = lax.all_to_all(packed, "sp_1", 0, 0, tiled=True)
    before, packed = pl.pallas_call(
        row_scan_kernel,
        name="row_scan",
        in_specs=[pl.BlockSpec(memory_space=pltpu.SMEM), whole(pieces.shape)],
        out_specs=[whole((STATE + 8, STATE)), whole((columns, PACKED, STATE))],
        out_shape=[
            jax.ShapeDtypeStruct((STATE + 8, STATE), F32),
            jax.ShapeDtypeStruct((columns, PACKED, STATE), BF16),
        ],
        grid=(1,),
        compiler_params=limits(8),
    )(lax.axis_index("sp_1").astype(jnp.int32).reshape(1), pieces)
    pieces = lax.all_to_all(packed, "sp_0", 0, 0, tiled=True)
    branches = pl.pallas_call(
        finish_kernel,
        name="finish",
        in_specs=[
            pl.BlockSpec(memory_space=pltpu.SMEM),
            whole(pieces.shape),
            whole(before.shape),
            whole(y.shape),
            whole(reads.shape),
            whole(reach.shape),
            whole(gate.shape),
            whole(pool.shape),
            whole((1, STATE)),
        ],
        out_specs=whole((length, 2 * STATE)),
        out_shape=jax.ShapeDtypeStruct((length, 2 * STATE), BF16),
        grid=(1,),
        compiler_params=limits(16),
    )(
        lax.axis_index("sp_0").astype(jnp.int32).reshape(1),
        pieces,
        before,
        y,
        reads,
        reach,
        gate,
        pool,
        gated_norm_scale.reshape(1, STATE),
    )
    branches = lax.all_to_all(
        branches.reshape(members, own_rows, 2 * STATE), "tp", 0, 0, tiled=True
    )
    return pl.pallas_call(
        output_kernel,
        name="output",
        in_specs=[whole(branches.shape), pl.BlockSpec(memory_space=pltpu.HBM)],
        out_specs=whole((own_rows, width)),
        out_shape=jax.ShapeDtypeStruct((own_rows, width), BF16),
        scratch_shapes=[
            pltpu.VMEM((members, 2 * STATE, width), BF16),
            pltpu.SemaphoreType.DMA((members,)),
        ],
        grid=(1,),
        compiler_params=limits(20),
    )(branches, in_hbm(output_weights))


def solution(mesh):
    ranges = mesh.shape["sp"]
    inner = 8 if ranges % 8 == 0 else 2
    torus = Mesh(mesh.devices.reshape(ranges // inner, inner, mesh.shape["tp"]), SP_TP)
    in_specs = (
        P(SP_TP, None),
        P(),
        P(None, "tp"),
        P(None, "tp"),
        P(None, "tp"),
        P(None, "tp"),
        P(),
        P(None, "tp"),
        P(None, "tp"),
        P(None, "tp"),
        P(None, "tp"),
        P(),
        P("tp", SP),
        P("tp", SP),
        P("tp"),
        P("tp", None, None),
        P("tp"),
        P("tp", None),
        P("tp", None),
    )
    return jax.shard_map(
        shards, mesh=torus, in_specs=in_specs, out_specs=P(SP_TP, None), check_vma=False
    )
```

```python
import jax
import jax.numpy as jnp
from jax import lax
from jax.experimental import pallas as pl
from jax.experimental.pallas import tpu as pltpu
from jax.sharding import Mesh
from jax.sharding import PartitionSpec as P

HEAD_DIM = 64
STATE = 128
BLOCK = 128
POOL_DIM = 64
HALO = 16
SP = ("sp_0", "sp_1")
TP = ("x", "core")
SP_TP = ("sp_0", "sp_1", "x", "core")
EPS = 1e-06
F32 = jnp.float32
BF16 = jnp.bfloat16
STEP_ROWS = 256
PACKED = STATE + 16


def silu(x):
    return x / (1.0 + jnp.exp(-x))


def by_head(first, second, shape):
    lane = lax.broadcasted_iota(jnp.int32, shape, len(shape) - 1)
    return jnp.where(lane < HEAD_DIM, first, second)


def norm_kernel(x_ref, scale_ref, out_ref, tail_ref):
    rows = normalize(x_ref[...], scale_ref[...])
    out_ref[...] = rows
    tail_ref[...] = rows[rows.shape[0] - HALO :]


def prepare_kernel(
    place_ref,
    rate_ref,
    value_ref,
    write_ref,
    read_ref,
    pool_ref,
    gate_ref,
    step_ref,
    value_taps_ref,
    write_taps_ref,
    read_taps_ref,
    bias_ref,
    pld_ref,
    group_ref,
    channel_ref,
    state_output_ref,
    pool_output_ref,
    w_ref,
    taps_ref,
    lanes_ref,
    pool_matrix_ref,
    output_ref,
):
    rank = place_ref[1] * 2 + place_ref[2]
    heads, length = bias_ref.shape
    for k, ref in enumerate((value_ref, write_ref, read_ref, pool_ref, gate_ref)):
        w_ref[:, k * STATE : (k + 1) * STATE] = ref[...]
    shape = (step_ref.shape[1], STATE)
    row, lane = (lax.broadcasted_iota(jnp.int32, shape, k) for k in range(2))
    chosen = jnp.where((lane < heads) & (row == rank * heads + lane), 1.0, 0.0).astype(BF16)
    w_ref[:, 5 * STATE :] = jnp.dot(
        step_ref[...], chosen, preferred_element_type=F32
    ).astype(BF16)
    for k, ref in enumerate((value_taps_ref, write_taps_ref, read_taps_ref)):
        taps_ref[0:4, k * STATE : (k + 1) * STATE] = ref[...]
    blocks = length // BLOCK
    pairs = heads * blocks
    for b in range(blocks):
        at = slice(b * BLOCK, (b + 1) * BLOCK)
        lanes_ref[b * heads : (b + 1) * heads] = bias_ref[:, at]
        lanes_ref[pairs + b * heads : pairs + (b + 1) * heads] = pld_ref[:, at]
    odd = lax.broadcasted_iota(jnp.int32, (pairs, BLOCK), 0) % 2 == 1
    lanes_ref[2 * pairs : 3 * pairs] = jnp.exp(
        jnp.where(odd, rate_ref[rank * heads + 1], rate_ref[rank * heads])
    )
    at_lane = lax.broadcasted_iota(jnp.int32, (1, STATE), 1)
    level = (rank * 2 + at_lane // POOL_DIM) % 4
    window = jnp.where(
        level == 0, 2.0, jnp.where(level == 1, 4.0, jnp.where(level == 2, 8.0, 16.0))
    )
    lanes_ref[3 * pairs : 3 * pairs + 1] = window
    lanes_ref[3 * pairs + 1 : 3 * pairs + 2] = channel_ref[...]
    shape = (POOL_DIM, STATE)
    row, lane = (lax.broadcasted_iota(jnp.int32, shape, k) for k in range(2))
    for k in range(2):
        place = jnp.where(lane == row + k * POOL_DIM, 1.0, 0.0).astype(BF16)
        pool_matrix_ref[k * POOL_DIM : (k + 1) * POOL_DIM] = jnp.dot(
            group_ref[k], place, preferred_element_type=F32
        ).astype(BF16)
    count = state_output_ref.shape[0]
    output_ref[:count] = state_output_ref[...]
    output_ref[count:] = pool_output_ref[...]


def halves_kernel(prior_ref, next_ref, first_ref, second_ref):
    half = first_ref.shape[0]
    first_ref[...] = prior_ref[:half]
    second_ref[...] = next_ref[half:]


def project_kernel(*refs):
    *row_refs, w_ref, other_ref, own_out, other_out, rows_ref = refs
    at = 0
    tails = [ref[...] for ref in row_refs if ref.shape[0] == HALO]
    for ref in row_refs:
        if ref.shape[0] != HALO:
            rows_ref[at : at + ref.shape[0]] = ref[...]
            at += ref.shape[0]
    if tails:
        tail = tails[0]
        for other in tails[1:]:
            tail = tail + other
        rows_ref[at:] = tail
    rows = rows_ref[...]
    own_out[...] = jnp.dot(rows, w_ref[...], preferred_element_type=F32).astype(BF16)
    other_out[...] = jnp.dot(rows, other_ref[...], preferred_element_type=F32).astype(BF16)


def mix_kernel(
    place_ref,
    own_near_ref,
    own_far_ref,
    other_near_ref,
    other_far_ref,
    taps_ref,
    lanes_ref,
    pool_matrix_ref,
    y_ref,
    reads_ref,
    reach_ref,
    gate_ref,
    pool_ref,
    state_ref,
    conv_in,
    pool_in,
    step_in,
    mixed_ref,
):
    length = y_ref.shape[0]
    chunks = length // STEP_ROWS
    blocks = length // BLOCK
    pairs = 2 * blocks
    bias, pld, rate = (lanes_ref[k * pairs : (k + 1) * pairs] for k in range(3))
    window = lanes_ref[3 * pairs : 3 * pairs + 1]
    pool_scale = lanes_ref[3 * pairs + 1 : 3 * pairs + 2]
    base, x, core = place_ref[0], place_ref[1], place_ref[2]
    near = own_near_ref.shape[0] - HALO
    halo = jnp.where(
        core == 0, own_near_ref[near:].astype(F32), other_near_ref[near:].astype(F32)
    )
    conv_in[:HALO] = halo[:, : 3 * STATE]
    pool_in[:HALO] = halo[:, 3 * STATE : 4 * STATE]
    ring = blocks // 2
    for side, near_ref, far_ref in ((core, own_near_ref, own_far_ref), (1 - core, other_near_ref, other_far_ref)):
        for away, source in ((0, near_ref[:BLOCK]), (ring - 1, near_ref[BLOCK : 2 * BLOCK]), (1, near_ref[2 * BLOCK : 3 * BLOCK]), (2, far_ref[...])):
            first = pl.multiple_of(((x + away) % ring * 2 + side) * BLOCK, BLOCK)
            wide = source.astype(F32)
            conv_in[pl.ds(HALO + first, BLOCK)] = wide[:, : 3 * STATE]
            pool_in[pl.ds(HALO + first, BLOCK)] = wide[:, 3 * STATE : 4 * STATE]
            gate_ref[pl.ds(first, BLOCK)] = silu(wide[:, 4 * STATE : 5 * STATE])
            step_in[pl.ds(first, BLOCK)] = wide[:, 5 * STATE :]
    for c in range(chunks):
        first = c * STEP_ROWS
        at = slice(first, first + STEP_ROWS)
        reached = slice(first, first + HALO + STEP_ROWS)
        extended = conv_in[reached]
        summed = extended * taps_ref[3:4, :]
        for back in range(1, 4):
            summed = summed + pltpu.roll(extended, back, 0) * taps_ref[3 - back : 4 - back, :]
        convolved = silu(summed[HALO:]).astype(BF16)
        mixed_ref[at] = convolved[:, : 2 * STATE]
        reads_ref[at] = convolved[:, 2 * STATE :]

        wide = pool_in[reached]
        sum_two = wide + pltpu.roll(wide, 1, 0)
        sum_four = sum_two + pltpu.roll(sum_two, 2, 0)
        sum_eight = sum_four + pltpu.roll(sum_four, 4, 0)
        sum_sixteen = sum_eight + pltpu.roll(sum_eight, 8, 0)
        window_sum = jnp.where(
            window == 2.0,
            sum_two,
            jnp.where(window == 4.0, sum_four, jnp.where(window == 8.0, sum_eight, sum_sixteen)),
        )[HALO:]
        position = (
            base + first + 1 + lax.broadcasted_iota(jnp.int32, (STEP_ROWS, 1), 0)
        ).astype(F32)
        difference = (window_sum / jnp.minimum(position, window) - wide[HALO:]).astype(BF16)
        pooled = jnp.dot(difference, pool_matrix_ref[...], preferred_element_type=F32)
        pool_ref[at] = (pooled * pool_scale).astype(BF16)

    square = (BLOCK, BLOCK)
    row_at = lax.broadcasted_iota(jnp.int32, square, 0)
    col_at = lax.broadcasted_iota(jnp.int32, square, 1)
    upper = (row_at <= col_at).astype(F32)
    causal = row_at >= col_at
    spread = step_in[:BLOCK]
    for b in range(1, blocks):
        spread = spread + pltpu.roll(step_in[b * BLOCK : (b + 1) * BLOCK], 2 * b, 1)
    step = jax.nn.softplus(spread.T[:pairs] + bias)
    cum = jnp.dot(
        pld - rate * step,
        upper,
        precision=lax.Precision.HIGHEST,
        preferred_element_type=F32,
    )
    total = jnp.broadcast_to(cum[:, BLOCK - 1 :], (pairs, BLOCK))
    prefix = jnp.zeros((2, BLOCK), F32)
    prefixes = []
    for b in range(blocks):
        prefixes.append(prefix)
        prefix = prefix + total[2 * b : 2 * b + 2]
    columns = jnp.concatenate(
        [
            cum,
            jnp.exp(total - cum) * step,
            jnp.exp(cum),
            jnp.exp(jnp.concatenate(prefixes, axis=0) + cum),
            jnp.zeros((BLOCK - 4 * pairs, BLOCK), F32),
        ],
        axis=0,
    ).T

    def column(kind, b, h):
        j = kind * pairs + 2 * b + h
        return columns[:, j : j + 1]

    carried = jnp.zeros((STATE, STATE), F32)
    for b in range(blocks):
        at = slice(b * BLOCK, (b + 1) * BLOCK)
        values = mixed_ref[at, :STATE]
        writes = mixed_ref[at, STATE:]
        reads = reads_ref[at]
        affinity = lax.dot_general(
            reads, writes, (((1,), (1,)), ((), ())), preferred_element_type=F32
        )
        inside = []
        for h in range(2):
            row = 2 * b + h
            spacing = column(0, b, h) - cum[row : row + 1]
            within = affinity * jnp.exp(jnp.where(causal, spacing, -jnp.inf)) * step[row : row + 1]
            inside.append(jnp.dot(within.astype(BF16), values, preferred_element_type=F32))
        weighted = (
            values.astype(F32) * by_head(column(1, b, 0), column(1, b, 1), square)
        ).astype(BF16)
        contrib = lax.dot_general(
            writes, weighted, (((0,), (0,)), ((), ())), preferred_element_type=F32
        )
        local = jnp.dot(reads, carried.astype(BF16), preferred_element_type=F32)
        y_ref[at] = by_head(inside[0], inside[1], square) + local * by_head(
            column(2, b, 0), column(2, b, 1), square
        )
        reach_ref[at] = by_head(column(3, b, 0), column(3, b, 1), square)
        decay = by_head(total[2 * b : 2 * b + 1], total[2 * b + 1 : 2 * b + 2], (1, STATE))
        carried = carried * jnp.exp(decay) + contrib
    packed = pack(carried, by_head(prefix[0:1], prefix[1:2], (1, STATE)))
    for k in range(state_ref.shape[0]):
        state_ref[k] = packed


def pack(state, total):
    high = total.astype(BF16)
    low = (total - high.astype(F32)).astype(BF16)
    row = lax.broadcasted_iota(jnp.int32, (PACKED - STATE, STATE), 0)
    tail = jnp.where(row == 0, high.astype(F32), jnp.where(row == 1, low.astype(F32), 0.0))
    return jnp.concatenate([state.astype(BF16), tail.astype(BF16)], axis=0)


def scan_pieces(pieces_ref, here):
    state = before_state = jnp.zeros((STATE, STATE), F32)
    total = before_total = jnp.zeros((1, STATE), F32)
    for k in range(pieces_ref.shape[0]):
        tail = pieces_ref[k, STATE:, :].astype(F32)
        decay = tail[0:1, :] + tail[1:2, :]
        state = state * jnp.exp(decay) + pieces_ref[k, :STATE, :].astype(F32)
        total = total + decay
        passed = k < here
        before_state = jnp.where(passed, state, before_state)
        before_total = jnp.where(passed, total, before_total)
    return state, total, before_state, before_total


def row_scan_kernel(here_ref, pieces_ref, before_ref, packed_ref):
    state, total, before_state, before_total = scan_pieces(pieces_ref, here_ref[0])
    before_ref[:STATE, :] = before_state
    before_ref[STATE:, :] = jnp.broadcast_to(before_total, (8, STATE))
    packed = pack(state, total)
    for k in range(packed_ref.shape[0]):
        packed_ref[k] = packed


def finish_kernel(
    here_ref,
    pieces_ref,
    before_ref,
    y_ref,
    reads_ref,
    reach_ref,
    gate_ref,
    pool_ref,
    scale_ref,
    out_ref,
):
    _, _, rows_before, _ = scan_pieces(pieces_ref, here_ref[0])
    incoming = rows_before * jnp.exp(before_ref[STATE : STATE + 1, :]) + before_ref[:STATE, :]
    crossed = jnp.dot(reads_ref[...], incoming.astype(BF16), preferred_element_type=F32)
    gated = (y_ref[...] + crossed * reach_ref[...]) * gate_ref[...]
    norm = lax.rsqrt(jnp.mean(gated * gated, axis=-1, keepdims=True) + EPS)
    out_ref[:, :STATE] = (gated * norm * scale_ref[...]).astype(BF16)
    out_ref[:, STATE:] = pool_ref[...]


def output_kernel(place_ref, rows_ref, own_ref, prior_ref, next_ref, far_a_ref, far_b_ref, keep_ref, send_ref, total_ref):
    x, core = place_ref[1], place_ref[2]
    ring = rows_ref.shape[0]
    half = far_a_ref.shape[0]
    total = jnp.dot(rows_ref[x], own_ref[...], preferred_element_type=F32)
    total = total + jnp.dot(rows_ref[(x + ring - 1) % ring], prior_ref[...], preferred_element_type=F32)
    total = total + jnp.dot(rows_ref[(x + 1) % ring], next_ref[...], preferred_element_type=F32)
    far = rows_ref[(x + 2) % ring]
    total = total + jnp.dot(far[:, :half], far_a_ref[...], preferred_element_type=F32)
    total_ref[...] = total + jnp.dot(far[:, half:], far_b_ref[...], preferred_element_type=F32)
    count = keep_ref.shape[0]
    keep_ref[...] = total_ref[pl.ds(pl.multiple_of(core * count, count), count)]
    send_ref[...] = total_ref[pl.ds(pl.multiple_of((1 - core) * count, count), count)].astype(BF16)


def join_kernel(keep_ref, other_ref, out_ref):
    out_ref[...] = (keep_ref[...] + other_ref[...].astype(F32)).astype(BF16)


def limits(mebibytes):
    return pltpu.CompilerParams(vmem_limit_bytes=mebibytes * 2**20)


def whole(shape):
    return pl.BlockSpec(shape, lambda *_: (0,) * len(shape))


def normalize(rows, scale):
    wide = rows.astype(F32)
    return (wide * lax.rsqrt(jnp.mean(wide * wide, axis=-1, keepdims=True) + EPS) * scale).astype(
        BF16
    )


def rows_before(rows, ring):
    ranges = lax.axis_size(SP)
    members = 2 * ring
    return [
        lax.ppermute(
            rows,
            SP_TP,
            [(i * members + members - 1, (i + 1) * members + 2 * k) for i in range(ranges - 1)],
        )
        for k in range(ring)
    ]


def around(array, away):
    ring = lax.axis_size("x")
    return lax.ppermute(array, "x", [(i, (i + away) % ring) for i in range(ring)])


def swapped(array):
    return lax.ppermute(array, "core", [(0, 1), (1, 0)])


def kernel_call(body, out_shape, *arrays, scratch=(), mebibytes=16):
    def spec(array):
        if array.ndim == 1:
            return pl.BlockSpec(memory_space=pltpu.SMEM)
        return whole(array.shape)

    return pl.pallas_call(
        body,
        grid=(1,),
        in_specs=[spec(array) for array in arrays],
        out_specs=jax.tree.map(lambda out: whole(out.shape), out_shape),
        out_shape=out_shape,
        scratch_shapes=list(scratch),
        compiler_params=limits(mebibytes),
    )(*arrays)


def held(shape, dtype):
    return jax.ShapeDtypeStruct(shape, dtype)


def shards(
    activations,
    input_norm_scale,
    value_weight_matrix,
    gate_weight_matrix,
    write_weight_matrix,
    read_weight_matrix,
    step_weight_matrix,
    pooling_input_matrix,
    value_filter_weight,
    write_filter_weight,
    read_filter_weight,
    head_log_decay_rate,
    step_bias_offset,
    position_log_decay,
    gated_norm_scale,
    pooling_group_matrix,
    pooling_channel_scale,
    state_output_matrix,
    pooling_output_matrix,
):
    x, core = lax.axis_index("x"), lax.axis_index("core")
    ring = lax.axis_size("x")
    sp_rank = lax.axis_index(SP)
    own_rows, width = activations.shape
    length = own_rows * ring * 2
    blocks = length // BLOCK
    scale = input_norm_scale.reshape(1, width)

    place = jnp.stack([sp_rank * length, x, core]).astype(jnp.int32)
    normed, tail = kernel_call(
        norm_kernel, [held((own_rows, width), BF16), held((HALO, width), BF16)], activations, scale
    )
    prior = around(normed, 1)
    following = around(normed, -1)
    found = rows_before(tail, ring)
    output_rows = state_output_matrix.shape[0] + pooling_output_matrix.shape[0]
    weights, taps, lanes, pool_matrix, own_output = kernel_call(
        prepare_kernel,
        [
            held((width, 6 * STATE), BF16),
            held((8, 3 * STATE), F32),
            held((6 * blocks + 8, STATE), F32),
            held((STATE, STATE), BF16),
            held((output_rows, width), BF16),
        ],
        place,
        head_log_decay_rate,
        value_weight_matrix,
        write_weight_matrix,
        read_weight_matrix,
        pooling_input_matrix,
        gate_weight_matrix,
        step_weight_matrix,
        value_filter_weight,
        write_filter_weight,
        read_filter_weight,
        step_bias_offset,
        position_log_decay,
        pooling_group_matrix,
        pooling_channel_scale.reshape(1, STATE),
        state_output_matrix,
        pooling_output_matrix,
        mebibytes=24,
    )
    other_weights = swapped(weights)
    half = own_rows // 2
    far = kernel_call(halves_kernel, [held((half, width), BF16)] * 2, prior, following)
    far_first = around(far[0], 1)
    far_second = around(far[1], -1)

    def project(*pieces):
        count = sum(piece.shape[0] for piece in pieces if piece.shape[0] > HALO)
        count += HALO * any(piece.shape[0] == HALO for piece in pieces)
        return kernel_call(
            project_kernel,
            [held((count, weights.shape[1]), BF16)] * 2,
            *pieces,
            weights,
            other_weights,
            scratch=[pltpu.VMEM((count, width), BF16)],
            mebibytes=24,
        )

    own_near, send_near = project(normed, prior, following, *found)
    other_near = swapped(send_near)
    own_far, send_far = project(far_first, far_second)
    other_far = swapped(send_far)

    columns, inner = lax.axis_size("sp_0"), lax.axis_size("sp_1")
    y, reads, reach, gate, pool, packed = kernel_call(
        mix_kernel,
        [
            held((length, STATE), F32),
            held((length, STATE), BF16),
            held((length, STATE), F32),
            held((length, STATE), F32),
            held((length, STATE), BF16),
            held((inner, PACKED, STATE), BF16),
        ],
        place,
        own_near,
        own_far,
        other_near,
        other_far,
        taps,
        lanes,
        pool_matrix,
        scratch=[
            pltpu.VMEM((HALO + length, 3 * STATE), F32),
            pltpu.VMEM((HALO + length, STATE), F32),
            pltpu.VMEM((length, STATE), F32),
            pltpu.VMEM((length, 2 * STATE), BF16),
        ],
        mebibytes=24,
    )

    packed, own_output = lax.optimization_barrier((packed, own_output))
    prior_output = around(own_output, 1)
    next_output = around(own_output, -1)
    pieces = lax.all_to_all(packed, "sp_1", 0, 0, tiled=True)
    before, packed = kernel_call(
        row_scan_kernel,
        [held((STATE + 8, STATE), F32), held((columns, PACKED, STATE), BF16)],
        lax.axis_index("sp_1").astype(jnp.int32).reshape(1),
        pieces,
        mebibytes=8,
    )
    pieces = lax.all_to_all(packed, "sp_0", 0, 0, tiled=True)
    prior_output, next_output, pieces = lax.optimization_barrier(
        (prior_output, next_output, pieces)
    )
    half = output_rows // 2
    far = kernel_call(halves_kernel, [held((half, width), BF16)] * 2, prior_output, next_output)
    far_output = (around(far[0], 1), around(far[1], -1))
    branches = kernel_call(
        finish_kernel,
        held((length, 2 * STATE), BF16),
        lax.axis_index("sp_0").astype(jnp.int32).reshape(1),
        pieces,
        before,
        y,
        reads,
        reach,
        gate,
        pool,
        gated_norm_scale.reshape(1, STATE),
    )
    branches = lax.all_to_all(
        branches.reshape(ring, 2 * own_rows, 2 * STATE), "x", 0, 0, tiled=True
    )
    keep, send = kernel_call(
        output_kernel,
        [held((own_rows, width), F32), held((own_rows, width), BF16)],
        place,
        branches,
        own_output,
        prior_output,
        next_output,
        *far_output,
        scratch=[pltpu.VMEM((2 * own_rows, width), F32)],
        mebibytes=24,
    )
    return kernel_call(join_kernel, held((own_rows, width), BF16), keep, swapped(send), mebibytes=8)


def solution(mesh):
    ranges = mesh.shape["sp"]
    inner = 8 if ranges % 8 == 0 else 2
    shape = (ranges // inner, inner, mesh.shape["tp"] // 2, 2)
    torus = Mesh(mesh.devices.reshape(shape), SP_TP)
    in_specs = (
        P(SP_TP, None),
        P(),
        P(None, TP),
        P(None, TP),
        P(None, TP),
        P(None, TP),
        P(),
        P(None, TP),
        P(None, TP),
        P(None, TP),
        P(None, TP),
        P(),
        P(TP, SP),
        P(TP, SP),
        P(TP),
        P(TP, None, None),
        P(TP),
        P(TP, None),
        P(TP, None),
    )

    return jax.shard_map(
        shards, mesh=torus, in_specs=in_specs, out_specs=P(SP_TP, None), check_vma=False
    )
```

```python
import jax
import jax.numpy as jnp
from jax import lax
from jax.experimental import pallas as pl
from jax.experimental.pallas import tpu as pltpu
from jax.sharding import Mesh
from jax.sharding import PartitionSpec as P

HEAD_DIM = 64
STATE = 128
BLOCK = 128
POOL_DIM = 64
HALO = 16
SP = ("sp_0", "sp_1")
TP = ("x", "core")
SP_TP = ("sp_0", "sp_1", "x", "core")
EPS = 1e-06
F32 = jnp.float32
BF16 = jnp.bfloat16
STEP_ROWS = 256
PACKED = STATE + 16


def silu(x):
    return x / (1.0 + jnp.exp(-x))


def by_head(first, second, shape):
    lane = lax.broadcasted_iota(jnp.int32, shape, len(shape) - 1)
    return jnp.where(lane < HEAD_DIM, first, second)


def fetch(pairs, arrived):
    copies = [
        pltpu.make_async_copy(source, target, arrived.at[k])
        for k, (source, target) in enumerate(pairs)
    ]
    for copy in copies:
        copy.start()
    for copy in copies:
        copy.wait()


def norm_kernel(x_hbm, scale_hbm, out_ref, tail_ref, x_ref, scale_ref, arrived):
    fetch(((x_hbm, x_ref), (scale_hbm, scale_ref)), arrived)
    rows = normalize(x_ref[...], scale_ref[...])
    out_ref[...] = rows
    tail_ref[...] = rows[rows.shape[0] - HALO :]


def prepare_kernel(
    place_ref,
    value_hbm,
    write_hbm,
    read_hbm,
    pool_hbm,
    gate_hbm,
    state_output_hbm,
    pool_output_hbm,
    *refs,
):
    small_hbm, (w_ref, output_hbm, taps_ref, lanes_ref, pool_matrix_ref), small = (
        refs[:9],
        refs[9:14],
        refs[14:23],
    )
    arrived = refs[23]
    step_ref, value_taps, write_taps, read_taps, bias_ref, pld_ref, rate_ref = small[:7]
    group_ref, channel_ref = small[7:]
    count = state_output_hbm.shape[0]
    large = [
        (ref, w_ref.at[:, k * STATE : (k + 1) * STATE])
        for k, ref in enumerate((value_hbm, write_hbm, read_hbm, pool_hbm, gate_hbm))
    ]
    large.append((state_output_hbm, output_hbm.at[:count]))
    large.append((pool_output_hbm, output_hbm.at[count:]))
    fetch(large + list(zip(small_hbm, small)), arrived)
    rank = place_ref[1] * 2 + place_ref[2]
    heads, length = bias_ref.shape
    shape = (step_ref.shape[0], STATE)
    row, lane = (lax.broadcasted_iota(jnp.int32, shape, k) for k in range(2))
    chosen = jnp.where((lane < heads) & (row == rank * heads + lane), 1.0, 0.0).astype(BF16)
    w_ref[:, 5 * STATE :] = lax.dot_general(
        step_ref[...], chosen, (((0,), (0,)), ((), ())), preferred_element_type=F32
    ).astype(BF16)
    for k, ref in enumerate((value_taps, write_taps, read_taps)):
        taps_ref[0:4, k * STATE : (k + 1) * STATE] = ref[...]
    blocks = length // BLOCK
    pairs = heads * blocks
    for b in range(blocks):
        at = slice(b * BLOCK, (b + 1) * BLOCK)
        lanes_ref[b * heads : (b + 1) * heads] = bias_ref[:, at]
        lanes_ref[pairs + b * heads : pairs + (b + 1) * heads] = pld_ref[:, at]
    rates = rate_ref[...]
    at_head = lax.broadcasted_iota(jnp.int32, rates.shape, 1)
    own = [
        jnp.sum(jnp.where(at_head == rank * heads + h, rates, 0.0), axis=1, keepdims=True)
        for h in range(2)
    ]
    odd = lax.broadcasted_iota(jnp.int32, (pairs, BLOCK), 0) % 2 == 1
    lanes_ref[2 * pairs : 3 * pairs] = jnp.exp(jnp.where(odd, own[1], own[0]))
    at_lane = lax.broadcasted_iota(jnp.int32, (1, STATE), 1)
    level = (rank * 2 + at_lane // POOL_DIM) % 4
    window = jnp.where(
        level == 0, 2.0, jnp.where(level == 1, 4.0, jnp.where(level == 2, 8.0, 16.0))
    )
    lanes_ref[3 * pairs : 3 * pairs + 1] = window
    lanes_ref[3 * pairs + 1 : 3 * pairs + 2] = channel_ref[...]
    shape = (POOL_DIM, STATE)
    row, lane = (lax.broadcasted_iota(jnp.int32, shape, k) for k in range(2))
    for k in range(2):
        place = jnp.where(lane == row + k * POOL_DIM, 1.0, 0.0).astype(BF16)
        pool_matrix_ref[k * POOL_DIM : (k + 1) * POOL_DIM] = jnp.dot(
            group_ref[k], place, preferred_element_type=F32
        ).astype(BF16)


def halves_kernel(prior_ref, next_ref, first_ref, second_ref):
    half = first_ref.shape[0]
    first_ref[...] = prior_ref[:half]
    second_ref[...] = next_ref[half:]


def project_kernel(*refs):
    *row_refs, w_ref, other_ref, own_out, other_out, rows_ref = refs
    at = 0
    tails = [ref[...] for ref in row_refs if ref.shape[0] == HALO]
    for ref in row_refs:
        if ref.shape[0] != HALO:
            rows_ref[at : at + ref.shape[0]] = ref[...]
            at += ref.shape[0]
    if tails:
        tail = tails[0]
        for other in tails[1:]:
            tail = tail + other
        rows_ref[at:] = tail
    rows = rows_ref[...]
    own_out[...] = jnp.dot(rows, w_ref[...], preferred_element_type=F32).astype(BF16)
    other_out[...] = jnp.dot(rows, other_ref[...], preferred_element_type=F32).astype(BF16)


def mix_kernel(
    place_ref,
    own_near_ref,
    own_far_ref,
    other_near_ref,
    other_far_ref,
    taps_ref,
    lanes_ref,
    pool_matrix_ref,
    y_ref,
    reads_ref,
    reach_ref,
    gate_ref,
    pool_ref,
    state_ref,
    conv_in,
    pool_in,
    step_in,
    mixed_ref,
):
    length = y_ref.shape[0]
    chunks = length // STEP_ROWS
    blocks = length // BLOCK
    pairs = 2 * blocks
    bias, pld, rate = (lanes_ref[k * pairs : (k + 1) * pairs] for k in range(3))
    window = lanes_ref[3 * pairs : 3 * pairs + 1]
    pool_scale = lanes_ref[3 * pairs + 1 : 3 * pairs + 2]
    base, x, core = place_ref[0], place_ref[1], place_ref[2]
    near = own_near_ref.shape[0] - HALO
    halo = jnp.where(
        core == 0, own_near_ref[near:].astype(F32), other_near_ref[near:].astype(F32)
    )
    conv_in[:HALO] = halo[:, : 3 * STATE]
    pool_in[:HALO] = halo[:, 3 * STATE : 4 * STATE]
    ring = blocks // 2
    for side, near_ref, far_ref in ((core, own_near_ref, own_far_ref), (1 - core, other_near_ref, other_far_ref)):
        for away, source in ((0, near_ref[:BLOCK]), (ring - 1, near_ref[BLOCK : 2 * BLOCK]), (1, near_ref[2 * BLOCK : 3 * BLOCK]), (2, far_ref[...])):
            first = pl.multiple_of(((x + away) % ring * 2 + side) * BLOCK, BLOCK)
            wide = source.astype(F32)
            conv_in[pl.ds(HALO + first, BLOCK)] = wide[:, : 3 * STATE]
            pool_in[pl.ds(HALO + first, BLOCK)] = wide[:, 3 * STATE : 4 * STATE]
            gate_ref[pl.ds(first, BLOCK)] = silu(wide[:, 4 * STATE : 5 * STATE])
            step_in[pl.ds(first, BLOCK)] = wide[:, 5 * STATE :]
    for c in range(chunks):
        first = c * STEP_ROWS
        at = slice(first, first + STEP_ROWS)
        reached = slice(first, first + HALO + STEP_ROWS)
        extended = conv_in[reached]
        summed = extended * taps_ref[3:4, :]
        for back in range(1, 4):
            summed = summed + pltpu.roll(extended, back, 0) * taps_ref[3 - back : 4 - back, :]
        convolved = silu(summed[HALO:]).astype(BF16)
        mixed_ref[at] = convolved[:, : 2 * STATE]
        reads_ref[at] = convolved[:, 2 * STATE :]

        wide = pool_in[reached]
        sum_two = wide + pltpu.roll(wide, 1, 0)
        sum_four = sum_two + pltpu.roll(sum_two, 2, 0)
        sum_eight = sum_four + pltpu.roll(sum_four, 4, 0)
        sum_sixteen = sum_eight + pltpu.roll(sum_eight, 8, 0)
        window_sum = jnp.where(
            window == 2.0,
            sum_two,
            jnp.where(window == 4.0, sum_four, jnp.where(window == 8.0, sum_eight, sum_sixteen)),
        )[HALO:]
        position = (
            base + first + 1 + lax.broadcasted_iota(jnp.int32, (STEP_ROWS, 1), 0)
        ).astype(F32)
        difference = (window_sum / jnp.minimum(position, window) - wide[HALO:]).astype(BF16)
        pooled = jnp.dot(difference, pool_matrix_ref[...], preferred_element_type=F32)
        pool_ref[at] = (pooled * pool_scale).astype(BF16)

    square = (BLOCK, BLOCK)
    row_at = lax.broadcasted_iota(jnp.int32, square, 0)
    col_at = lax.broadcasted_iota(jnp.int32, square, 1)
    upper = (row_at <= col_at).astype(F32)
    causal = row_at >= col_at
    spread = step_in[:BLOCK]
    for b in range(1, blocks):
        spread = spread + pltpu.roll(step_in[b * BLOCK : (b + 1) * BLOCK], 2 * b, 1)
    step = jax.nn.softplus(spread.T[:pairs] + bias)
    cum = jnp.dot(
        pld - rate * step,
        upper,
        precision=lax.Precision.HIGHEST,
        preferred_element_type=F32,
    )
    total = jnp.broadcast_to(cum[:, BLOCK - 1 :], (pairs, BLOCK))
    prefix = jnp.zeros((2, BLOCK), F32)
    prefixes = []
    for b in range(blocks):
        prefixes.append(prefix)
        prefix = prefix + total[2 * b : 2 * b + 2]
    columns = jnp.concatenate(
        [
            cum,
            jnp.exp(total - cum) * step,
            jnp.exp(cum),
            jnp.exp(jnp.concatenate(prefixes, axis=0) + cum),
            jnp.zeros((BLOCK - 4 * pairs, BLOCK), F32),
        ],
        axis=0,
    ).T

    def column(kind, b, h):
        j = kind * pairs + 2 * b + h
        return columns[:, j : j + 1]

    carried = jnp.zeros((STATE, STATE), F32)
    for b in range(blocks):
        at = slice(b * BLOCK, (b + 1) * BLOCK)
        values = mixed_ref[at, :STATE]
        writes = mixed_ref[at, STATE:]
        reads = reads_ref[at]
        affinity = lax.dot_general(
            reads, writes, (((1,), (1,)), ((), ())), preferred_element_type=F32
        )
        inside = []
        for h in range(2):
            row = 2 * b + h
            spacing = column(0, b, h) - cum[row : row + 1]
            within = affinity * jnp.exp(jnp.where(causal, spacing, -jnp.inf)) * step[row : row + 1]
            inside.append(jnp.dot(within.astype(BF16), values, preferred_element_type=F32))
        weighted = (
            values.astype(F32) * by_head(column(1, b, 0), column(1, b, 1), square)
        ).astype(BF16)
        contrib = lax.dot_general(
            writes, weighted, (((0,), (0,)), ((), ())), preferred_element_type=F32
        )
        local = jnp.dot(reads, carried.astype(BF16), preferred_element_type=F32)
        y_ref[at] = by_head(inside[0], inside[1], square) + local * by_head(
            column(2, b, 0), column(2, b, 1), square
        )
        reach_ref[at] = by_head(column(3, b, 0), column(3, b, 1), square)
        decay = by_head(total[2 * b : 2 * b + 1], total[2 * b + 1 : 2 * b + 2], (1, STATE))
        carried = carried * jnp.exp(decay) + contrib
    packed = pack(carried, by_head(prefix[0:1], prefix[1:2], (1, STATE)))
    for k in range(state_ref.shape[0]):
        state_ref[k] = packed


def pack(state, total):
    high = total.astype(BF16)
    low = (total - high.astype(F32)).astype(BF16)
    row = lax.broadcasted_iota(jnp.int32, (PACKED - STATE, STATE), 0)
    tail = jnp.where(row == 0, high.astype(F32), jnp.where(row == 1, low.astype(F32), 0.0))
    return jnp.concatenate([state.astype(BF16), tail.astype(BF16)], axis=0)


def scan_pieces(pieces_ref, here):
    state = before_state = jnp.zeros((STATE, STATE), F32)
    total = before_total = jnp.zeros((1, STATE), F32)
    for k in range(pieces_ref.shape[0]):
        tail = pieces_ref[k, STATE:, :].astype(F32)
        decay = tail[0:1, :] + tail[1:2, :]
        state = state * jnp.exp(decay) + pieces_ref[k, :STATE, :].astype(F32)
        total = total + decay
        passed = k < here
        before_state = jnp.where(passed, state, before_state)
        before_total = jnp.where(passed, total, before_total)
    return state, total, before_state, before_total


def row_scan_kernel(here_ref, pieces_ref, before_ref, packed_ref):
    state, total, before_state, before_total = scan_pieces(pieces_ref, here_ref[0])
    before_ref[:STATE, :] = before_state
    before_ref[STATE:, :] = jnp.broadcast_to(before_total, (8, STATE))
    packed = pack(state, total)
    for k in range(packed_ref.shape[0]):
        packed_ref[k] = packed


def finish_kernel(
    here_ref,
    pieces_ref,
    before_ref,
    y_ref,
    reads_ref,
    reach_ref,
    gate_ref,
    pool_ref,
    scale_ref,
    out_ref,
):
    _, _, rows_before, _ = scan_pieces(pieces_ref, here_ref[0])
    incoming = rows_before * jnp.exp(before_ref[STATE : STATE + 1, :]) + before_ref[:STATE, :]
    crossed = jnp.dot(reads_ref[...], incoming.astype(BF16), preferred_element_type=F32)
    gated = (y_ref[...] + crossed * reach_ref[...]) * gate_ref[...]
    norm = lax.rsqrt(jnp.mean(gated * gated, axis=-1, keepdims=True) + EPS)
    out_ref[:, :STATE] = (gated * norm * scale_ref[...]).astype(BF16)
    out_ref[:, STATE:] = pool_ref[...]


def output_kernel(rows_ref, w_ref, out_ref, weights_ref, arrived):
    parts = rows_ref.shape[0]
    incoming = [
        pltpu.make_async_copy(w_ref.at[k], weights_ref.at[k], arrived.at[k]) for k in range(parts)
    ]
    for copy in incoming:
        copy.start()
    total = None
    for k in range(parts):
        incoming[k].wait()
        part = jnp.dot(rows_ref[k], weights_ref[k], preferred_element_type=F32)
        total = part if total is None else total + part
    out_ref[...] = total.astype(BF16)


def limits(mebibytes):
    return pltpu.CompilerParams(vmem_limit_bytes=mebibytes * 2**20)


def whole(shape):
    return pl.BlockSpec(shape, lambda *_: (0,) * len(shape))


def normalize(rows, scale):
    wide = rows.astype(F32)
    return (wide * lax.rsqrt(jnp.mean(wide * wide, axis=-1, keepdims=True) + EPS) * scale).astype(
        BF16
    )


def rows_before(rows, ring):
    ranges = lax.axis_size(SP)
    members = 2 * ring
    return [
        lax.ppermute(
            rows,
            SP_TP,
            [(i * members + members - 1, (i + 1) * members + 2 * k) for i in range(ranges - 1)],
        )
        for k in range(ring)
    ]


def around(array, away):
    ring = lax.axis_size("x")
    return lax.ppermute(array, "x", [(i, (i + away) % ring) for i in range(ring)])


def swapped(array):
    return lax.ppermute(array, "core", [(0, 1), (1, 0)])


class Stored:
    def __init__(self, array):
        self.array = pltpu.with_memory_space_constraint(array, pltpu.HBM)
        self.shape, self.dtype = array.shape, array.dtype


def kernel_call(body, out_shape, *arrays, scratch=(), mebibytes=16, stored_outputs=()):
    def spec(array):
        if isinstance(array, Stored):
            return pl.BlockSpec(memory_space=pltpu.HBM)
        if array.ndim == 1:
            return pl.BlockSpec(memory_space=pltpu.SMEM)
        return whole(array.shape)

    return pl.pallas_call(
        body,
        grid=(1,),
        in_specs=[spec(array) for array in arrays],
        out_specs=[
            pl.BlockSpec(memory_space=pltpu.HBM) if k in stored_outputs else whole(out.shape)
            for k, out in enumerate(out_shape)
        ],
        out_shape=out_shape,
        scratch_shapes=list(scratch),
        compiler_params=limits(mebibytes),
    )(*(array.array if isinstance(array, Stored) else array for array in arrays))


def held(shape, dtype):
    return jax.ShapeDtypeStruct(shape, dtype)


def shards(
    activations,
    input_norm_scale,
    value_weight_matrix,
    gate_weight_matrix,
    write_weight_matrix,
    read_weight_matrix,
    step_weight_matrix,
    pooling_input_matrix,
    value_filter_weight,
    write_filter_weight,
    read_filter_weight,
    head_log_decay_rate,
    step_bias_offset,
    position_log_decay,
    gated_norm_scale,
    pooling_group_matrix,
    pooling_channel_scale,
    state_output_matrix,
    pooling_output_matrix,
):
    x, core = lax.axis_index("x"), lax.axis_index("core")
    ring = lax.axis_size("x")
    sp_rank = lax.axis_index(SP)
    own_rows, width = activations.shape
    length = own_rows * ring * 2
    blocks = length // BLOCK
    scale = input_norm_scale.reshape(1, width)

    place = jnp.stack([sp_rank * length, x, core]).astype(jnp.int32)
    normed, tail = kernel_call(
        norm_kernel,
        [held((own_rows, width), BF16), held((HALO, width), BF16)],
        Stored(activations),
        Stored(scale),
        scratch=[
            pltpu.VMEM((own_rows, width), BF16),
            pltpu.VMEM((1, width), F32),
            pltpu.SemaphoreType.DMA((2,)),
        ],
    )
    prior = around(normed, 1)
    following = around(normed, -1)
    found = rows_before(tail, ring)
    output_rows = state_output_matrix.shape[0] + pooling_output_matrix.shape[0]
    small = [
        step_weight_matrix.T,
        value_filter_weight,
        write_filter_weight,
        read_filter_weight,
        step_bias_offset,
        position_log_decay,
        head_log_decay_rate.reshape(1, -1),
        pooling_group_matrix,
        pooling_channel_scale.reshape(1, STATE),
    ]
    large = [
        value_weight_matrix,
        write_weight_matrix,
        read_weight_matrix,
        pooling_input_matrix,
        gate_weight_matrix,
        state_output_matrix,
        pooling_output_matrix,
    ]
    weights, own_output, taps, lanes, pool_matrix = kernel_call(
        prepare_kernel,
        [
            held((width, 6 * STATE), BF16),
            held((output_rows, width), BF16),
            held((8, 3 * STATE), F32),
            held((6 * blocks + 8, STATE), F32),
            held((STATE, STATE), BF16),
        ],
        place,
        *(Stored(array) for array in large + small),
        scratch=[pltpu.VMEM(array.shape, array.dtype) for array in small]
        + [pltpu.SemaphoreType.DMA((len(large) + len(small),))],
        stored_outputs=(1,),
    )
    other_weights = swapped(weights)
    half = own_rows // 2
    far = kernel_call(halves_kernel, [held((half, width), BF16)] * 2, prior, following)
    far_first = around(far[0], 1)
    far_second = around(far[1], -1)

    def project(*pieces):
        count = sum(piece.shape[0] for piece in pieces if piece.shape[0] > HALO)
        count += HALO * any(piece.shape[0] == HALO for piece in pieces)
        return kernel_call(
            project_kernel,
            [held((count, weights.shape[1]), BF16)] * 2,
            *pieces,
            weights,
            other_weights,
            scratch=[pltpu.VMEM((count, width), BF16)],
            mebibytes=24,
        )

    own_near, send_near = project(normed, prior, following, *found)
    other_near = swapped(send_near)
    own_far, send_far = project(far_first, far_second)
    own_far, own_output = lax.optimization_barrier((own_far, own_output))
    output_weights = lax.all_gather(own_output, TP, axis=0)
    other_far = swapped(send_far)

    columns, inner = lax.axis_size("sp_0"), lax.axis_size("sp_1")
    y, reads, reach, gate, pool, packed = kernel_call(
        mix_kernel,
        [
            held((length, STATE), F32),
            held((length, STATE), BF16),
            held((length, STATE), F32),
            held((length, STATE), F32),
            held((length, STATE), BF16),
            held((inner, PACKED, STATE), BF16),
        ],
        place,
        own_near,
        own_far,
        other_near,
        other_far,
        taps,
        lanes,
        pool_matrix,
        scratch=[
            pltpu.VMEM((HALO + length, 3 * STATE), F32),
            pltpu.VMEM((HALO + length, STATE), F32),
            pltpu.VMEM((length, STATE), F32),
            pltpu.VMEM((length, 2 * STATE), BF16),
        ],
        mebibytes=24,
    )

    pieces = lax.all_to_all(packed, "sp_1", 0, 0, tiled=True)
    before, packed = kernel_call(
        row_scan_kernel,
        [held((STATE + 8, STATE), F32), held((columns, PACKED, STATE), BF16)],
        lax.axis_index("sp_1").astype(jnp.int32).reshape(1),
        pieces,
        mebibytes=8,
    )
    pieces = lax.all_to_all(packed, "sp_0", 0, 0, tiled=True)
    (branches,) = kernel_call(
        finish_kernel,
        [held((length, 2 * STATE), BF16)],
        lax.axis_index("sp_0").astype(jnp.int32).reshape(1),
        pieces,
        before,
        y,
        reads,
        reach,
        gate,
        pool,
        gated_norm_scale.reshape(1, STATE),
    )
    members = 2 * ring
    branches = lax.all_to_all(
        branches.reshape(members, own_rows, 2 * STATE), TP, 0, 0, tiled=True
    )
    (mixed,) = kernel_call(
        output_kernel,
        [held((own_rows, width), BF16)],
        branches,
        Stored(output_weights),
        scratch=[
            pltpu.VMEM((members, 2 * STATE, width), BF16),
            pltpu.SemaphoreType.DMA((members,)),
        ],
        mebibytes=20,
    )
    return mixed


def solution(mesh):
    ranges = mesh.shape["sp"]
    inner = 8 if ranges % 8 == 0 else 2
    shape = (ranges // inner, inner, mesh.shape["tp"] // 2, 2)
    torus = Mesh(mesh.devices.reshape(shape), SP_TP)
    in_specs = (
        P(SP_TP, None),
        P(),
        P(None, TP),
        P(None, TP),
        P(None, TP),
        P(None, TP),
        P(),
        P(None, TP),
        P(None, TP),
        P(None, TP),
        P(None, TP),
        P(),
        P(TP, SP),
        P(TP, SP),
        P(TP),
        P(TP, None, None),
        P(TP),
        P(TP, None),
        P(TP, None),
    )

    return jax.shard_map(
        shards, mesh=torus, in_specs=in_specs, out_specs=P(SP_TP, None), check_vma=False
    )
```

```python
import jax
import jax.numpy as jnp
from jax import lax
from jax.experimental import pallas as pl
from jax.experimental.pallas import tpu as pltpu
from jax.sharding import Mesh
from jax.sharding import PartitionSpec as P

HEAD_DIM = 64
STATE = 128
BLOCK = 128
POOL_DIM = 64
HALO = 16
SP = ("sp_0", "sp_1")
TP = ("x", "core")
SP_TP = ("sp_0", "sp_1", "x", "core")
EPS = 1e-06
F32 = jnp.float32
BF16 = jnp.bfloat16
STEP_ROWS = 256
PACKED = STATE + 16


def silu(x):
    return x / (1.0 + jnp.exp(-x))


def by_head(first, second, shape):
    lane = lax.broadcasted_iota(jnp.int32, shape, len(shape) - 1)
    return jnp.where(lane < HEAD_DIM, first, second)


def fetch(pairs, arrived):
    copies = [
        pltpu.make_async_copy(source, target, arrived.at[k])
        for k, (source, target) in enumerate(pairs)
    ]
    for copy in copies:
        copy.start()
    for copy in copies:
        copy.wait()


def norm_kernel(x_hbm, scale_hbm, out_ref, tail_ref, x_ref, scale_ref, arrived):
    fetch(((x_hbm, x_ref), (scale_hbm, scale_ref)), arrived)
    rows = normalize(x_ref[...], scale_ref[...])
    out_ref[...] = rows
    tail_ref[...] = rows[rows.shape[0] - HALO :]


def prepare_kernel(
    place_ref,
    value_hbm,
    write_hbm,
    read_hbm,
    pool_hbm,
    gate_hbm,
    state_output_hbm,
    pool_output_hbm,
    *refs,
):
    small_hbm, (w_ref, output_ref, taps_ref, lanes_ref, pool_matrix_ref), small = (
        refs[:9],
        refs[9:14],
        refs[14:23],
    )
    arrived = refs[23]
    step_ref, value_taps, write_taps, read_taps, bias_ref, pld_ref, rate_ref = small[:7]
    group_ref, channel_ref = small[7:]
    count = state_output_hbm.shape[0]
    large = [
        (ref, w_ref.at[:, k * STATE : (k + 1) * STATE])
        for k, ref in enumerate((value_hbm, write_hbm, read_hbm, pool_hbm, gate_hbm))
    ]
    large.append((state_output_hbm, output_ref.at[:count]))
    large.append((pool_output_hbm, output_ref.at[count:]))
    fetch(large + list(zip(small_hbm, small)), arrived)
    rank = place_ref[1] * 2 + place_ref[2]
    heads, length = bias_ref.shape
    shape = (step_ref.shape[0], STATE)
    row, lane = (lax.broadcasted_iota(jnp.int32, shape, k) for k in range(2))
    chosen = jnp.where((lane < heads) & (row == rank * heads + lane), 1.0, 0.0).astype(BF16)
    w_ref[:, 5 * STATE :] = lax.dot_general(
        step_ref[...], chosen, (((0,), (0,)), ((), ())), preferred_element_type=F32
    ).astype(BF16)
    for k, ref in enumerate((value_taps, write_taps, read_taps)):
        taps_ref[0:4, k * STATE : (k + 1) * STATE] = ref[...]
    blocks = length // BLOCK
    pairs = heads * blocks
    for b in range(blocks):
        at = slice(b * BLOCK, (b + 1) * BLOCK)
        lanes_ref[b * heads : (b + 1) * heads] = bias_ref[:, at]
        lanes_ref[pairs + b * heads : pairs + (b + 1) * heads] = pld_ref[:, at]
    rates = rate_ref[...]
    at_head = lax.broadcasted_iota(jnp.int32, rates.shape, 1)
    own = [
        jnp.sum(jnp.where(at_head == rank * heads + h, rates, 0.0), axis=1, keepdims=True)
        for h in range(2)
    ]
    odd = lax.broadcasted_iota(jnp.int32, (pairs, BLOCK), 0) % 2 == 1
    lanes_ref[2 * pairs : 3 * pairs] = jnp.exp(jnp.where(odd, own[1], own[0]))
    at_lane = lax.broadcasted_iota(jnp.int32, (1, STATE), 1)
    level = (rank * 2 + at_lane // POOL_DIM) % 4
    window = jnp.where(
        level == 0, 2.0, jnp.where(level == 1, 4.0, jnp.where(level == 2, 8.0, 16.0))
    )
    lanes_ref[3 * pairs : 3 * pairs + 1] = window
    lanes_ref[3 * pairs + 1 : 3 * pairs + 2] = channel_ref[...]
    shape = (POOL_DIM, STATE)
    row, lane = (lax.broadcasted_iota(jnp.int32, shape, k) for k in range(2))
    for k in range(2):
        place = jnp.where(lane == row + k * POOL_DIM, 1.0, 0.0).astype(BF16)
        pool_matrix_ref[k * POOL_DIM : (k + 1) * POOL_DIM] = jnp.dot(
            group_ref[k], place, preferred_element_type=F32
        ).astype(BF16)


def halves_kernel(prior_ref, next_ref, first_ref, second_ref):
    half = first_ref.shape[0]
    first_ref[...] = prior_ref[:half]
    second_ref[...] = next_ref[half:]


def project_kernel(*refs):
    *row_refs, w_ref, other_ref, own_out, other_out, rows_ref = refs
    at = 0
    tails = [ref[...] for ref in row_refs if ref.shape[0] == HALO]
    for ref in row_refs:
        if ref.shape[0] != HALO:
            rows_ref[at : at + ref.shape[0]] = ref[...]
            at += ref.shape[0]
    if tails:
        tail = tails[0]
        for other in tails[1:]:
            tail = tail + other
        rows_ref[at:] = tail
    rows = rows_ref[...]
    own_out[...] = jnp.dot(rows, w_ref[...], preferred_element_type=F32).astype(BF16)
    other_out[...] = jnp.dot(rows, other_ref[...], preferred_element_type=F32).astype(BF16)


def mix_kernel(
    place_ref,
    own_near_ref,
    own_far_ref,
    other_near_ref,
    other_far_ref,
    taps_ref,
    lanes_ref,
    pool_matrix_ref,
    y_ref,
    reads_ref,
    reach_ref,
    gate_ref,
    pool_ref,
    state_ref,
    conv_in,
    pool_in,
    step_in,
    mixed_ref,
):
    length = y_ref.shape[0]
    chunks = length // STEP_ROWS
    blocks = length // BLOCK
    pairs = 2 * blocks
    bias, pld, rate = (lanes_ref[k * pairs : (k + 1) * pairs] for k in range(3))
    window = lanes_ref[3 * pairs : 3 * pairs + 1]
    pool_scale = lanes_ref[3 * pairs + 1 : 3 * pairs + 2]
    base, x, core = place_ref[0], place_ref[1], place_ref[2]
    near = own_near_ref.shape[0] - HALO
    halo = jnp.where(
        core == 0, own_near_ref[near:].astype(F32), other_near_ref[near:].astype(F32)
    )
    conv_in[:HALO] = halo[:, : 3 * STATE]
    pool_in[:HALO] = halo[:, 3 * STATE : 4 * STATE]
    ring = blocks // 2
    for side, near_ref, far_ref in ((core, own_near_ref, own_far_ref), (1 - core, other_near_ref, other_far_ref)):
        for away, source in ((0, near_ref[:BLOCK]), (ring - 1, near_ref[BLOCK : 2 * BLOCK]), (1, near_ref[2 * BLOCK : 3 * BLOCK]), (2, far_ref[...])):
            first = pl.multiple_of(((x + away) % ring * 2 + side) * BLOCK, BLOCK)
            wide = source.astype(F32)
            conv_in[pl.ds(HALO + first, BLOCK)] = wide[:, : 3 * STATE]
            pool_in[pl.ds(HALO + first, BLOCK)] = wide[:, 3 * STATE : 4 * STATE]
            gate_ref[pl.ds(first, BLOCK)] = silu(wide[:, 4 * STATE : 5 * STATE])
            step_in[pl.ds(first, BLOCK)] = wide[:, 5 * STATE :]
    for c in range(chunks):
        first = c * STEP_ROWS
        at = slice(first, first + STEP_ROWS)
        reached = slice(first, first + HALO + STEP_ROWS)
        extended = conv_in[reached]
        summed = extended * taps_ref[3:4, :]
        for back in range(1, 4):
            summed = summed + pltpu.roll(extended, back, 0) * taps_ref[3 - back : 4 - back, :]
        convolved = silu(summed[HALO:]).astype(BF16)
        mixed_ref[at] = convolved[:, : 2 * STATE]
        reads_ref[at] = convolved[:, 2 * STATE :]

        wide = pool_in[reached]
        sum_two = wide + pltpu.roll(wide, 1, 0)
        sum_four = sum_two + pltpu.roll(sum_two, 2, 0)
        sum_eight = sum_four + pltpu.roll(sum_four, 4, 0)
        sum_sixteen = sum_eight + pltpu.roll(sum_eight, 8, 0)
        window_sum = jnp.where(
            window == 2.0,
            sum_two,
            jnp.where(window == 4.0, sum_four, jnp.where(window == 8.0, sum_eight, sum_sixteen)),
        )[HALO:]
        position = (
            base + first + 1 + lax.broadcasted_iota(jnp.int32, (STEP_ROWS, 1), 0)
        ).astype(F32)
        difference = (window_sum / jnp.minimum(position, window) - wide[HALO:]).astype(BF16)
        pooled = jnp.dot(difference, pool_matrix_ref[...], preferred_element_type=F32)
        pool_ref[at] = (pooled * pool_scale).astype(BF16)

    square = (BLOCK, BLOCK)
    row_at = lax.broadcasted_iota(jnp.int32, square, 0)
    col_at = lax.broadcasted_iota(jnp.int32, square, 1)
    upper = (row_at <= col_at).astype(F32)
    causal = row_at >= col_at
    spread = step_in[:BLOCK]
    for b in range(1, blocks):
        spread = spread + pltpu.roll(step_in[b * BLOCK : (b + 1) * BLOCK], 2 * b, 1)
    step = jax.nn.softplus(spread.T[:pairs] + bias)
    cum = jnp.dot(
        pld - rate * step,
        upper,
        precision=lax.Precision.HIGHEST,
        preferred_element_type=F32,
    )
    total = jnp.broadcast_to(cum[:, BLOCK - 1 :], (pairs, BLOCK))
    prefix = jnp.zeros((2, BLOCK), F32)
    prefixes = []
    for b in range(blocks):
        prefixes.append(prefix)
        prefix = prefix + total[2 * b : 2 * b + 2]
    columns = jnp.concatenate(
        [
            cum,
            jnp.exp(total - cum) * step,
            jnp.exp(cum),
            jnp.exp(jnp.concatenate(prefixes, axis=0) + cum),
            jnp.zeros((BLOCK - 4 * pairs, BLOCK), F32),
        ],
        axis=0,
    ).T

    def column(kind, b, h):
        j = kind * pairs + 2 * b + h
        return columns[:, j : j + 1]

    carried = jnp.zeros((STATE, STATE), F32)
    for b in range(blocks):
        at = slice(b * BLOCK, (b + 1) * BLOCK)
        values = mixed_ref[at, :STATE]
        writes = mixed_ref[at, STATE:]
        reads = reads_ref[at]
        affinity = lax.dot_general(
            reads, writes, (((1,), (1,)), ((), ())), preferred_element_type=F32
        )
        inside = []
        for h in range(2):
            row = 2 * b + h
            spacing = column(0, b, h) - cum[row : row + 1]
            within = affinity * jnp.exp(jnp.where(causal, spacing, -jnp.inf)) * step[row : row + 1]
            inside.append(jnp.dot(within.astype(BF16), values, preferred_element_type=F32))
        weighted = (
            values.astype(F32) * by_head(column(1, b, 0), column(1, b, 1), square)
        ).astype(BF16)
        contrib = lax.dot_general(
            writes, weighted, (((0,), (0,)), ((), ())), preferred_element_type=F32
        )
        local = jnp.dot(reads, carried.astype(BF16), preferred_element_type=F32)
        y_ref[at] = by_head(inside[0], inside[1], square) + local * by_head(
            column(2, b, 0), column(2, b, 1), square
        )
        reach_ref[at] = by_head(column(3, b, 0), column(3, b, 1), square)
        decay = by_head(total[2 * b : 2 * b + 1], total[2 * b + 1 : 2 * b + 2], (1, STATE))
        carried = carried * jnp.exp(decay) + contrib
    packed = pack(carried, by_head(prefix[0:1], prefix[1:2], (1, STATE)))
    for k in range(state_ref.shape[0]):
        state_ref[k] = packed


def pack(state, total):
    high = total.astype(BF16)
    low = (total - high.astype(F32)).astype(BF16)
    row = lax.broadcasted_iota(jnp.int32, (PACKED - STATE, STATE), 0)
    tail = jnp.where(row == 0, high.astype(F32), jnp.where(row == 1, low.astype(F32), 0.0))
    return jnp.concatenate([state.astype(BF16), tail.astype(BF16)], axis=0)


def scan_pieces(pieces_ref, here):
    state = before_state = jnp.zeros((STATE, STATE), F32)
    total = before_total = jnp.zeros((1, STATE), F32)
    for k in range(pieces_ref.shape[0]):
        tail = pieces_ref[k, STATE:, :].astype(F32)
        decay = tail[0:1, :] + tail[1:2, :]
        state = state * jnp.exp(decay) + pieces_ref[k, :STATE, :].astype(F32)
        total = total + decay
        passed = k < here
        before_state = jnp.where(passed, state, before_state)
        before_total = jnp.where(passed, total, before_total)
    return state, total, before_state, before_total


def row_scan_kernel(here_ref, pieces_ref, before_ref, packed_ref):
    state, total, before_state, before_total = scan_pieces(pieces_ref, here_ref[0])
    before_ref[:STATE, :] = before_state
    before_ref[STATE:, :] = jnp.broadcast_to(before_total, (8, STATE))
    packed = pack(state, total)
    for k in range(packed_ref.shape[0]):
        packed_ref[k] = packed


def finish_kernel(
    here_ref,
    pieces_ref,
    before_ref,
    y_ref,
    reads_ref,
    reach_ref,
    gate_ref,
    pool_ref,
    scale_ref,
    out_ref,
):
    _, _, rows_before, _ = scan_pieces(pieces_ref, here_ref[0])
    incoming = rows_before * jnp.exp(before_ref[STATE : STATE + 1, :]) + before_ref[:STATE, :]
    crossed = jnp.dot(reads_ref[...], incoming.astype(BF16), preferred_element_type=F32)
    gated = (y_ref[...] + crossed * reach_ref[...]) * gate_ref[...]
    norm = lax.rsqrt(jnp.mean(gated * gated, axis=-1, keepdims=True) + EPS)
    out_ref[:, :STATE] = (gated * norm * scale_ref[...]).astype(BF16)
    out_ref[:, STATE:] = pool_ref[...]


def output_kernel(rows_ref, w_ref, out_ref, weights_ref, arrived):
    parts = rows_ref.shape[0]
    incoming = [
        pltpu.make_async_copy(w_ref.at[k], weights_ref.at[k], arrived.at[k]) for k in range(parts)
    ]
    for copy in incoming:
        copy.start()
    total = None
    for k in range(parts):
        incoming[k].wait()
        part = jnp.dot(rows_ref[k], weights_ref[k], preferred_element_type=F32)
        total = part if total is None else total + part
    out_ref[...] = total.astype(BF16)


def limits(mebibytes):
    return pltpu.CompilerParams(vmem_limit_bytes=mebibytes * 2**20)


def whole(shape):
    return pl.BlockSpec(shape, lambda *_: (0,) * len(shape))


def normalize(rows, scale):
    wide = rows.astype(F32)
    return (wide * lax.rsqrt(jnp.mean(wide * wide, axis=-1, keepdims=True) + EPS) * scale).astype(
        BF16
    )


def rows_before(rows, ring):
    ranges = lax.axis_size(SP)
    members = 2 * ring
    return [
        lax.ppermute(
            rows,
            SP_TP,
            [(i * members + members - 1, (i + 1) * members + 2 * k) for i in range(ranges - 1)],
        )
        for k in range(ring)
    ]


def around(array, away):
    ring = lax.axis_size("x")
    return lax.ppermute(array, "x", [(i, (i + away) % ring) for i in range(ring)])


def swapped(array):
    return lax.ppermute(array, "core", [(0, 1), (1, 0)])


class Stored:
    def __init__(self, array):
        self.array = pltpu.with_memory_space_constraint(array, pltpu.HBM)
        self.shape, self.dtype = array.shape, array.dtype


def kernel_call(body, out_shape, *arrays, scratch=(), mebibytes=16):
    def spec(array):
        if isinstance(array, Stored):
            return pl.BlockSpec(memory_space=pltpu.HBM)
        if array.ndim == 1:
            return pl.BlockSpec(memory_space=pltpu.SMEM)
        return whole(array.shape)

    return pl.pallas_call(
        body,
        grid=(1,),
        in_specs=[spec(array) for array in arrays],
        out_specs=[whole(out.shape) for out in out_shape],
        out_shape=out_shape,
        scratch_shapes=list(scratch),
        compiler_params=limits(mebibytes),
    )(*(array.array if isinstance(array, Stored) else array for array in arrays))


def held(shape, dtype):
    return jax.ShapeDtypeStruct(shape, dtype)


def shards(
    activations,
    input_norm_scale,
    value_weight_matrix,
    gate_weight_matrix,
    write_weight_matrix,
    read_weight_matrix,
    step_weight_matrix,
    pooling_input_matrix,
    value_filter_weight,
    write_filter_weight,
    read_filter_weight,
    head_log_decay_rate,
    step_bias_offset,
    position_log_decay,
    gated_norm_scale,
    pooling_group_matrix,
    pooling_channel_scale,
    state_output_matrix,
    pooling_output_matrix,
):
    x, core = lax.axis_index("x"), lax.axis_index("core")
    ring = lax.axis_size("x")
    sp_rank = lax.axis_index(SP)
    own_rows, width = activations.shape
    length = own_rows * ring * 2
    blocks = length // BLOCK
    scale = input_norm_scale.reshape(1, width)

    place = jnp.stack([sp_rank * length, x, core]).astype(jnp.int32)
    normed, tail = kernel_call(
        norm_kernel,
        [held((own_rows, width), BF16), held((HALO, width), BF16)],
        Stored(activations),
        Stored(scale),
        scratch=[
            pltpu.VMEM((own_rows, width), BF16),
            pltpu.VMEM((1, width), F32),
            pltpu.SemaphoreType.DMA((2,)),
        ],
    )
    prior = around(normed, 1)
    following = around(normed, -1)
    found = rows_before(tail, ring)
    output_rows = state_output_matrix.shape[0] + pooling_output_matrix.shape[0]
    small = [
        step_weight_matrix.T,
        value_filter_weight,
        write_filter_weight,
        read_filter_weight,
        step_bias_offset,
        position_log_decay,
        head_log_decay_rate.reshape(1, -1),
        pooling_group_matrix,
        pooling_channel_scale.reshape(1, STATE),
    ]
    large = [
        value_weight_matrix,
        write_weight_matrix,
        read_weight_matrix,
        pooling_input_matrix,
        gate_weight_matrix,
        state_output_matrix,
        pooling_output_matrix,
    ]
    weights, own_output, taps, lanes, pool_matrix = kernel_call(
        prepare_kernel,
        [
            held((width, 6 * STATE), BF16),
            held((output_rows, width), BF16),
            held((8, 3 * STATE), F32),
            held((6 * blocks + 8, STATE), F32),
            held((STATE, STATE), BF16),
        ],
        place,
        *(Stored(array) for array in large + small),
        scratch=[pltpu.VMEM(array.shape, array.dtype) for array in small]
        + [pltpu.SemaphoreType.DMA((len(large) + len(small),))],
    )
    other_weights = swapped(weights)
    half = own_rows // 2
    far = kernel_call(halves_kernel, [held((half, width), BF16)] * 2, prior, following)
    far_first = around(far[0], 1)
    far_second = around(far[1], -1)

    def project(*pieces):
        count = sum(piece.shape[0] for piece in pieces if piece.shape[0] > HALO)
        count += HALO * any(piece.shape[0] == HALO for piece in pieces)
        return kernel_call(
            project_kernel,
            [held((count, weights.shape[1]), BF16)] * 2,
            *pieces,
            weights,
            other_weights,
            scratch=[pltpu.VMEM((count, width), BF16)],
            mebibytes=24,
        )

    own_near, send_near = project(normed, prior, following, *found)
    other_near = swapped(send_near)
    own_far, send_far = project(far_first, far_second)
    own_far, own_output = lax.optimization_barrier((own_far, own_output))
    output_weights = lax.all_gather(own_output, TP, axis=0)
    other_far = swapped(send_far)

    columns, inner = lax.axis_size("sp_0"), lax.axis_size("sp_1")
    y, reads, reach, gate, pool, packed = kernel_call(
        mix_kernel,
        [
            held((length, STATE), F32),
            held((length, STATE), BF16),
            held((length, STATE), F32),
            held((length, STATE), F32),
            held((length, STATE), BF16),
            held((inner, PACKED, STATE), BF16),
        ],
        place,
        own_near,
        own_far,
        other_near,
        other_far,
        taps,
        lanes,
        pool_matrix,
        scratch=[
            pltpu.VMEM((HALO + length, 3 * STATE), F32),
            pltpu.VMEM((HALO + length, STATE), F32),
            pltpu.VMEM((length, STATE), F32),
            pltpu.VMEM((length, 2 * STATE), BF16),
        ],
        mebibytes=24,
    )

    pieces = lax.all_to_all(packed, "sp_1", 0, 0, tiled=True)
    before, packed = kernel_call(
        row_scan_kernel,
        [held((STATE + 8, STATE), F32), held((columns, PACKED, STATE), BF16)],
        lax.axis_index("sp_1").astype(jnp.int32).reshape(1),
        pieces,
        mebibytes=8,
    )
    pieces = lax.all_to_all(packed, "sp_0", 0, 0, tiled=True)
    (branches,) = kernel_call(
        finish_kernel,
        [held((length, 2 * STATE), BF16)],
        lax.axis_index("sp_0").astype(jnp.int32).reshape(1),
        pieces,
        before,
        y,
        reads,
        reach,
        gate,
        pool,
        gated_norm_scale.reshape(1, STATE),
    )
    members = 2 * ring
    branches = lax.all_to_all(
        branches.reshape(members, own_rows, 2 * STATE), TP, 0, 0, tiled=True
    )
    (mixed,) = kernel_call(
        output_kernel,
        [held((own_rows, width), BF16)],
        branches,
        Stored(output_weights),
        scratch=[
            pltpu.VMEM((members, 2 * STATE, width), BF16),
            pltpu.SemaphoreType.DMA((members,)),
        ],
        mebibytes=20,
    )
    return mixed


def solution(mesh):
    ranges = mesh.shape["sp"]
    inner = 8 if ranges % 8 == 0 else 2
    shape = (ranges // inner, inner, mesh.shape["tp"] // 2, 2)
    torus = Mesh(mesh.devices.reshape(shape), SP_TP)
    in_specs = (
        P(SP_TP, None),
        P(),
        P(None, TP),
        P(None, TP),
        P(None, TP),
        P(None, TP),
        P(),
        P(None, TP),
        P(None, TP),
        P(None, TP),
        P(None, TP),
        P(),
        P(TP, SP),
        P(TP, SP),
        P(TP),
        P(TP, None, None),
        P(TP),
        P(TP, None),
        P(TP, None),
    )

    return jax.shard_map(
        shards, mesh=torus, in_specs=in_specs, out_specs=P(SP_TP, None), check_vma=False
    )
```

```python
import jax
import jax.numpy as jnp
from jax import lax
from jax.experimental import pallas as pl
from jax.experimental.pallas import tpu as pltpu
from jax.sharding import Mesh
from jax.sharding import PartitionSpec as P

HEAD_DIM = 64
STATE = 128
BLOCK = 128
POOL_DIM = 64
HALO = 16
SP = ("sp_0", "sp_1")
TP = ("x", "core")
SP_TP = ("sp_0", "sp_1", "x", "core")
EPS = 1e-06
F32 = jnp.float32
BF16 = jnp.bfloat16
STEP_ROWS = 256
PACKED = STATE + 16


def silu(x):
    return x / (1.0 + jnp.exp(-x))


def by_head(first, second, shape):
    lane = lax.broadcasted_iota(jnp.int32, shape, len(shape) - 1)
    return jnp.where(lane < HEAD_DIM, first, second)


def fetch(pairs, arrived):
    copies = [
        pltpu.make_async_copy(source, target, arrived.at[k])
        for k, (source, target) in enumerate(pairs)
    ]
    for copy in copies:
        copy.start()
    for copy in copies:
        copy.wait()


def norm_kernel(x_hbm, scale_hbm, out_ref, tail_ref, x_ref, scale_ref, arrived):
    fetch(((x_hbm, x_ref), (scale_hbm, scale_ref)), arrived)
    rows = normalize(x_ref[...], scale_ref[...])
    out_ref[...] = rows
    tail_ref[...] = rows[rows.shape[0] - HALO :]


def prepare_kernel(
    place_ref,
    value_hbm,
    write_hbm,
    read_hbm,
    pool_hbm,
    gate_hbm,
    state_output_hbm,
    pool_output_hbm,
    *refs,
):
    small_hbm, (w_ref, output_ref, taps_ref, lanes_ref, pool_matrix_ref), small = (
        refs[:9],
        refs[9:14],
        refs[14:23],
    )
    arrived = refs[23]
    step_ref, value_taps, write_taps, read_taps, bias_ref, pld_ref, rate_ref = small[:7]
    group_ref, channel_ref = small[7:]
    count = state_output_hbm.shape[0]
    large = [
        (ref, w_ref.at[:, k * STATE : (k + 1) * STATE])
        for k, ref in enumerate((value_hbm, write_hbm, read_hbm, pool_hbm, gate_hbm))
    ]
    large.append((state_output_hbm, output_ref.at[:count]))
    large.append((pool_output_hbm, output_ref.at[count:]))
    fetch(large + list(zip(small_hbm, small)), arrived)
    rank = place_ref[1] * 2 + place_ref[2]
    heads, length = bias_ref.shape
    shape = (step_ref.shape[0], STATE)
    row, lane = (lax.broadcasted_iota(jnp.int32, shape, k) for k in range(2))
    chosen = jnp.where((lane < heads) & (row == rank * heads + lane), 1.0, 0.0).astype(BF16)
    w_ref[:, 5 * STATE :] = lax.dot_general(
        step_ref[...], chosen, (((0,), (0,)), ((), ())), preferred_element_type=F32
    ).astype(BF16)
    for k, ref in enumerate((value_taps, write_taps, read_taps)):
        taps_ref[0:4, k * STATE : (k + 1) * STATE] = ref[...]
    blocks = length // BLOCK
    pairs = heads * blocks
    for b in range(blocks):
        at = slice(b * BLOCK, (b + 1) * BLOCK)
        lanes_ref[b * heads : (b + 1) * heads] = bias_ref[:, at]
        lanes_ref[pairs + b * heads : pairs + (b + 1) * heads] = pld_ref[:, at]
    rates = rate_ref[...]
    at_head = lax.broadcasted_iota(jnp.int32, rates.shape, 1)
    own = [
        jnp.sum(jnp.where(at_head == rank * heads + h, rates, 0.0), axis=1, keepdims=True)
        for h in range(2)
    ]
    odd = lax.broadcasted_iota(jnp.int32, (pairs, BLOCK), 0) % 2 == 1
    lanes_ref[2 * pairs : 3 * pairs] = jnp.exp(jnp.where(odd, own[1], own[0]))
    at_lane = lax.broadcasted_iota(jnp.int32, (1, STATE), 1)
    level = (rank * 2 + at_lane // POOL_DIM) % 4
    window = jnp.where(
        level == 0, 2.0, jnp.where(level == 1, 4.0, jnp.where(level == 2, 8.0, 16.0))
    )
    lanes_ref[3 * pairs : 3 * pairs + 1] = window
    lanes_ref[3 * pairs + 1 : 3 * pairs + 2] = channel_ref[...]
    shape = (POOL_DIM, STATE)
    row, lane = (lax.broadcasted_iota(jnp.int32, shape, k) for k in range(2))
    for k in range(2):
        place = jnp.where(lane == row + k * POOL_DIM, 1.0, 0.0).astype(BF16)
        pool_matrix_ref[k * POOL_DIM : (k + 1) * POOL_DIM] = jnp.dot(
            group_ref[k], place, preferred_element_type=F32
        ).astype(BF16)


def first_half_kernel(rows_ref, half_ref):
    half_ref[...] = rows_ref[: half_ref.shape[0]]


def second_half_kernel(rows_ref, half_ref):
    half_ref[...] = rows_ref[half_ref.shape[0] :]


def project_kernel(*refs):
    *row_refs, w_ref, other_ref, own_out, other_out, rows_ref = refs
    at = 0
    tails = [ref[...] for ref in row_refs if ref.shape[0] == HALO]
    for ref in row_refs:
        if ref.shape[0] != HALO:
            rows_ref[at : at + ref.shape[0]] = ref[...]
            at += ref.shape[0]
    if tails:
        tail = tails[0]
        for other in tails[1:]:
            tail = tail + other
        rows_ref[at:] = tail
    rows = rows_ref[...]
    own_out[...] = jnp.dot(rows, w_ref[...], preferred_element_type=F32).astype(BF16)
    other_out[...] = jnp.dot(rows, other_ref[...], preferred_element_type=F32).astype(BF16)


def mix_kernel(
    place_ref,
    own_near_ref,
    own_far_ref,
    other_near_ref,
    other_far_ref,
    taps_ref,
    lanes_ref,
    pool_matrix_ref,
    y_ref,
    reads_ref,
    reach_ref,
    gate_ref,
    pool_ref,
    state_ref,
    conv_in,
    pool_in,
    step_in,
    mixed_ref,
):
    length = y_ref.shape[0]
    chunks = length // STEP_ROWS
    blocks = length // BLOCK
    pairs = 2 * blocks
    bias, pld, rate = (lanes_ref[k * pairs : (k + 1) * pairs] for k in range(3))
    window = lanes_ref[3 * pairs : 3 * pairs + 1]
    pool_scale = lanes_ref[3 * pairs + 1 : 3 * pairs + 2]
    base, x, core = place_ref[0], place_ref[1], place_ref[2]
    near = own_near_ref.shape[0] - HALO
    halo = jnp.where(
        core == 0, own_near_ref[near:].astype(F32), other_near_ref[near:].astype(F32)
    )
    conv_in[:HALO] = halo[:, : 3 * STATE]
    pool_in[:HALO] = halo[:, 3 * STATE : 4 * STATE]
    ring = blocks // 2
    for side, near_ref, far_ref in (
        (core, own_near_ref, own_far_ref),
        (1 - core, other_near_ref, other_far_ref),
    ):
        ahead = ring + 1 - 2 * side
        behind = ring - 1 + 2 * side
        for away, source in (
            (0, near_ref[:BLOCK]),
            (behind, near_ref[BLOCK : 2 * BLOCK]),
            (ahead, near_ref[2 * BLOCK : 3 * BLOCK]),
            (2, far_ref[...]),
        ):
            first = pl.multiple_of(((x + away) % ring * 2 + side) * BLOCK, BLOCK)
            wide = source.astype(F32)
            conv_in[pl.ds(HALO + first, BLOCK)] = wide[:, : 3 * STATE]
            pool_in[pl.ds(HALO + first, BLOCK)] = wide[:, 3 * STATE : 4 * STATE]
            gate_ref[pl.ds(first, BLOCK)] = silu(wide[:, 4 * STATE : 5 * STATE])
            step_in[pl.ds(first, BLOCK)] = wide[:, 5 * STATE :]
    for c in range(chunks):
        first = c * STEP_ROWS
        at = slice(first, first + STEP_ROWS)
        reached = slice(first, first + HALO + STEP_ROWS)
        extended = conv_in[reached]
        summed = extended * taps_ref[3:4, :]
        for back in range(1, 4):
            summed = summed + pltpu.roll(extended, back, 0) * taps_ref[3 - back : 4 - back, :]
        convolved = silu(summed[HALO:]).astype(BF16)
        mixed_ref[at] = convolved[:, : 2 * STATE]
        reads_ref[at] = convolved[:, 2 * STATE :]

        wide = pool_in[reached]
        sum_two = wide + pltpu.roll(wide, 1, 0)
        sum_four = sum_two + pltpu.roll(sum_two, 2, 0)
        sum_eight = sum_four + pltpu.roll(sum_four, 4, 0)
        sum_sixteen = sum_eight + pltpu.roll(sum_eight, 8, 0)
        window_sum = jnp.where(
            window == 2.0,
            sum_two,
            jnp.where(window == 4.0, sum_four, jnp.where(window == 8.0, sum_eight, sum_sixteen)),
        )[HALO:]
        position = (
            base + first + 1 + lax.broadcasted_iota(jnp.int32, (STEP_ROWS, 1), 0)
        ).astype(F32)
        difference = (window_sum / jnp.minimum(position, window) - wide[HALO:]).astype(BF16)
        pooled = jnp.dot(difference, pool_matrix_ref[...], preferred_element_type=F32)
        pool_ref[at] = (pooled * pool_scale).astype(BF16)

    square = (BLOCK, BLOCK)
    row_at = lax.broadcasted_iota(jnp.int32, square, 0)
    col_at = lax.broadcasted_iota(jnp.int32, square, 1)
    upper = (row_at <= col_at).astype(F32)
    causal = row_at >= col_at
    spread = step_in[:BLOCK]
    for b in range(1, blocks):
        spread = spread + pltpu.roll(step_in[b * BLOCK : (b + 1) * BLOCK], 2 * b, 1)
    step = jax.nn.softplus(spread.T[:pairs] + bias)
    cum = jnp.dot(
        pld - rate * step,
        upper,
        precision=lax.Precision.HIGHEST,
        preferred_element_type=F32,
    )
    total = jnp.broadcast_to(cum[:, BLOCK - 1 :], (pairs, BLOCK))
    prefix = jnp.zeros((2, BLOCK), F32)
    prefixes = []
    for b in range(blocks):
        prefixes.append(prefix)
        prefix = prefix + total[2 * b : 2 * b + 2]
    columns = jnp.concatenate(
        [
            cum,
            jnp.exp(total - cum) * step,
            jnp.exp(cum),
            jnp.exp(jnp.concatenate(prefixes, axis=0) + cum),
            jnp.zeros((BLOCK - 4 * pairs, BLOCK), F32),
        ],
        axis=0,
    ).T

    def column(kind, b, h):
        j = kind * pairs + 2 * b + h
        return columns[:, j : j + 1]

    carried = jnp.zeros((STATE, STATE), F32)
    for b in range(blocks):
        at = slice(b * BLOCK, (b + 1) * BLOCK)
        values = mixed_ref[at, :STATE]
        writes = mixed_ref[at, STATE:]
        reads = reads_ref[at]
        affinity = lax.dot_general(
            reads, writes, (((1,), (1,)), ((), ())), preferred_element_type=F32
        )
        inside = []
        for h in range(2):
            row = 2 * b + h
            spacing = column(0, b, h) - cum[row : row + 1]
            within = affinity * jnp.exp(jnp.where(causal, spacing, -jnp.inf)) * step[row : row + 1]
            inside.append(jnp.dot(within.astype(BF16), values, preferred_element_type=F32))
        weighted = (
            values.astype(F32) * by_head(column(1, b, 0), column(1, b, 1), square)
        ).astype(BF16)
        contrib = lax.dot_general(
            writes, weighted, (((0,), (0,)), ((), ())), preferred_element_type=F32
        )
        local = jnp.dot(reads, carried.astype(BF16), preferred_element_type=F32)
        y_ref[at] = by_head(inside[0], inside[1], square) + local * by_head(
            column(2, b, 0), column(2, b, 1), square
        )
        reach_ref[at] = by_head(column(3, b, 0), column(3, b, 1), square)
        decay = by_head(total[2 * b : 2 * b + 1], total[2 * b + 1 : 2 * b + 2], (1, STATE))
        carried = carried * jnp.exp(decay) + contrib
    packed = pack(carried, by_head(prefix[0:1], prefix[1:2], (1, STATE)))
    for k in range(state_ref.shape[0]):
        state_ref[k] = packed


def pack(state, total):
    high = total.astype(BF16)
    low = (total - high.astype(F32)).astype(BF16)
    row = lax.broadcasted_iota(jnp.int32, (PACKED - STATE, STATE), 0)
    tail = jnp.where(row == 0, high.astype(F32), jnp.where(row == 1, low.astype(F32), 0.0))
    return jnp.concatenate([state.astype(BF16), tail.astype(BF16)], axis=0)


def scan_pieces(pieces_ref, here):
    state = before_state = jnp.zeros((STATE, STATE), F32)
    total = before_total = jnp.zeros((1, STATE), F32)
    for k in range(pieces_ref.shape[0]):
        tail = pieces_ref[k, STATE:, :].astype(F32)
        decay = tail[0:1, :] + tail[1:2, :]
        state = state * jnp.exp(decay) + pieces_ref[k, :STATE, :].astype(F32)
        total = total + decay
        passed = k < here
        before_state = jnp.where(passed, state, before_state)
        before_total = jnp.where(passed, total, before_total)
    return state, total, before_state, before_total


def row_scan_kernel(here_ref, pieces_ref, before_ref, packed_ref):
    state, total, before_state, before_total = scan_pieces(pieces_ref, here_ref[0])
    before_ref[:STATE, :] = before_state
    before_ref[STATE:, :] = jnp.broadcast_to(before_total, (8, STATE))
    packed = pack(state, total)
    for k in range(packed_ref.shape[0]):
        packed_ref[k] = packed


def finish_kernel(
    here_ref,
    pieces_ref,
    before_ref,
    y_ref,
    reads_ref,
    reach_ref,
    gate_ref,
    pool_ref,
    scale_ref,
    out_ref,
):
    _, _, rows_before, _ = scan_pieces(pieces_ref, here_ref[0])
    incoming = rows_before * jnp.exp(before_ref[STATE : STATE + 1, :]) + before_ref[:STATE, :]
    crossed = jnp.dot(reads_ref[...], incoming.astype(BF16), preferred_element_type=F32)
    gated = (y_ref[...] + crossed * reach_ref[...]) * gate_ref[...]
    norm = lax.rsqrt(jnp.mean(gated * gated, axis=-1, keepdims=True) + EPS)
    out_ref[:, :STATE] = (gated * norm * scale_ref[...]).astype(BF16)
    out_ref[:, STATE:] = pool_ref[...]


def output_kernel(
    place_ref,
    rows_ref,
    own_ref,
    behind_ref,
    ahead_ref,
    far_first_ref,
    far_second_ref,
    keep_ref,
    send_ref,
    total_ref,
):
    x, core = place_ref[1], place_ref[2]
    ring = rows_ref.shape[0]
    half = far_first_ref.shape[0]
    total = jnp.dot(rows_ref[x], own_ref[...], preferred_element_type=F32)
    behind = rows_ref[(x + ring - 1 + 2 * core) % ring]
    total = total + jnp.dot(behind, behind_ref[...], preferred_element_type=F32)
    ahead = rows_ref[(x + ring + 1 - 2 * core) % ring]
    total = total + jnp.dot(ahead, ahead_ref[...], preferred_element_type=F32)
    far = rows_ref[(x + 2) % ring]
    total = total + jnp.dot(far[:, :half], far_first_ref[...], preferred_element_type=F32)
    total_ref[...] = total + jnp.dot(
        far[:, half:], far_second_ref[...], preferred_element_type=F32
    )
    count = keep_ref.shape[0]
    keep_ref[...] = total_ref[pl.ds(pl.multiple_of(core * count, count), count)]
    send_ref[...] = total_ref[pl.ds(pl.multiple_of((1 - core) * count, count), count)].astype(BF16)


def join_kernel(keep_ref, other_ref, out_ref):
    out_ref[...] = (keep_ref[...] + other_ref[...].astype(F32)).astype(BF16)


def limits(mebibytes):
    return pltpu.CompilerParams(vmem_limit_bytes=mebibytes * 2**20)


def whole(shape):
    return pl.BlockSpec(shape, lambda *_: (0,) * len(shape))


def normalize(rows, scale):
    wide = rows.astype(F32)
    return (wide * lax.rsqrt(jnp.mean(wide * wide, axis=-1, keepdims=True) + EPS) * scale).astype(
        BF16
    )


def rows_before(rows, ring):
    ranges = lax.axis_size(SP)
    members = 2 * ring
    return [
        lax.ppermute(
            rows,
            SP_TP,
            [(i * members + members - 1, (i + 1) * members + 2 * k) for i in range(ranges - 1)],
        )
        for k in range(ring)
    ]


def around(array, away):
    ring = lax.axis_size("x")
    route = [
        (2 * i + side, 2 * ((i + away * (1 - 2 * side)) % ring) + side)
        for i in range(ring)
        for side in range(2)
    ]
    return lax.ppermute(array, TP, route)


def swapped(array):
    return lax.ppermute(array, "core", [(0, 1), (1, 0)])


class Stored:
    def __init__(self, array):
        self.array = pltpu.with_memory_space_constraint(array, pltpu.HBM)
        self.shape, self.dtype = array.shape, array.dtype


def kernel_call(body, out_shape, *arrays, scratch=(), mebibytes=16):
    def spec(array):
        if isinstance(array, Stored):
            return pl.BlockSpec(memory_space=pltpu.HBM)
        if array.ndim == 1:
            return pl.BlockSpec(memory_space=pltpu.SMEM)
        return whole(array.shape)

    return pl.pallas_call(
        body,
        grid=(1,),
        in_specs=[spec(array) for array in arrays],
        out_specs=[whole(out.shape) for out in out_shape],
        out_shape=out_shape,
        scratch_shapes=list(scratch),
        compiler_params=limits(mebibytes),
    )(*(array.array if isinstance(array, Stored) else array for array in arrays))


def held(shape, dtype):
    return jax.ShapeDtypeStruct(shape, dtype)


def shards(
    activations,
    input_norm_scale,
    value_weight_matrix,
    gate_weight_matrix,
    write_weight_matrix,
    read_weight_matrix,
    step_weight_matrix,
    pooling_input_matrix,
    value_filter_weight,
    write_filter_weight,
    read_filter_weight,
    head_log_decay_rate,
    step_bias_offset,
    position_log_decay,
    gated_norm_scale,
    pooling_group_matrix,
    pooling_channel_scale,
    state_output_matrix,
    pooling_output_matrix,
):
    x, core = lax.axis_index("x"), lax.axis_index("core")
    ring = lax.axis_size("x")
    sp_rank = lax.axis_index(SP)
    own_rows, width = activations.shape
    length = own_rows * ring * 2
    blocks = length // BLOCK
    scale = input_norm_scale.reshape(1, width)

    place = jnp.stack([sp_rank * length, x, core]).astype(jnp.int32)
    normed, tail = kernel_call(
        norm_kernel,
        [held((own_rows, width), BF16), held((HALO, width), BF16)],
        Stored(activations),
        Stored(scale),
        scratch=[
            pltpu.VMEM((own_rows, width), BF16),
            pltpu.VMEM((1, width), F32),
            pltpu.SemaphoreType.DMA((2,)),
        ],
    )
    prior = around(normed, 1)
    following = around(normed, -1)
    found = rows_before(tail, ring)
    output_rows = state_output_matrix.shape[0] + pooling_output_matrix.shape[0]
    small = [
        step_weight_matrix.T,
        value_filter_weight,
        write_filter_weight,
        read_filter_weight,
        step_bias_offset,
        position_log_decay,
        head_log_decay_rate.reshape(1, -1),
        pooling_group_matrix,
        pooling_channel_scale.reshape(1, STATE),
    ]
    large = [
        value_weight_matrix,
        write_weight_matrix,
        read_weight_matrix,
        pooling_input_matrix,
        gate_weight_matrix,
        state_output_matrix,
        pooling_output_matrix,
    ]
    weights, own_output, taps, lanes, pool_matrix = kernel_call(
        prepare_kernel,
        [
            held((width, 6 * STATE), BF16),
            held((output_rows, width), BF16),
            held((8, 3 * STATE), F32),
            held((6 * blocks + 8, STATE), F32),
            held((STATE, STATE), BF16),
        ],
        place,
        *(Stored(array) for array in large + small),
        scratch=[pltpu.VMEM(array.shape, array.dtype) for array in small]
        + [pltpu.SemaphoreType.DMA((len(large) + len(small),))],
    )
    other_weights = swapped(weights)
    half = own_rows // 2
    half_rows = [held((half, width), BF16)]
    (prior_half,) = kernel_call(first_half_kernel, half_rows, prior)
    far_first = around(prior_half, 1)
    (next_half,) = kernel_call(second_half_kernel, half_rows, following)
    far_second = around(next_half, -1)

    def project(*pieces):
        count = sum(piece.shape[0] for piece in pieces if piece.shape[0] > HALO)
        count += HALO * any(piece.shape[0] == HALO for piece in pieces)
        return kernel_call(
            project_kernel,
            [held((count, weights.shape[1]), BF16)] * 2,
            *pieces,
            weights,
            other_weights,
            scratch=[pltpu.VMEM((count, width), BF16)],
            mebibytes=24,
        )

    own_near, send_near = project(normed, prior, following, *found)
    other_near = swapped(send_near)
    own_far, send_far = project(far_first, far_second)
    send_far, own_output = lax.optimization_barrier((send_far, own_output))
    other_far = swapped(send_far)
    output_behind = around(own_output, 1)

    columns, inner = lax.axis_size("sp_0"), lax.axis_size("sp_1")
    y, reads, reach, gate, pool, packed = kernel_call(
        mix_kernel,
        [
            held((length, STATE), F32),
            held((length, STATE), BF16),
            held((length, STATE), F32),
            held((length, STATE), F32),
            held((length, STATE), BF16),
            held((inner, PACKED, STATE), BF16),
        ],
        place,
        own_near,
        own_far,
        other_near,
        other_far,
        taps,
        lanes,
        pool_matrix,
        scratch=[
            pltpu.VMEM((HALO + length, 3 * STATE), F32),
            pltpu.VMEM((HALO + length, STATE), F32),
            pltpu.VMEM((length, STATE), F32),
            pltpu.VMEM((length, 2 * STATE), BF16),
        ],
        mebibytes=24,
    )

    pieces = lax.all_to_all(packed, "sp_1", 0, 0, tiled=True)
    pieces, own_output = lax.optimization_barrier((pieces, own_output))
    output_ahead = around(own_output, -1)
    before, packed = kernel_call(
        row_scan_kernel,
        [held((STATE + 8, STATE), F32), held((columns, PACKED, STATE), BF16)],
        lax.axis_index("sp_1").astype(jnp.int32).reshape(1),
        pieces,
        mebibytes=8,
    )
    packed, output_behind = lax.optimization_barrier((packed, output_behind))
    pieces = lax.all_to_all(packed, "sp_0", 0, 0, tiled=True)
    output_behind, output_ahead, pieces = lax.optimization_barrier(
        (output_behind, output_ahead, pieces)
    )
    half_outputs = [held((output_rows // 2, width), BF16)]
    (half,) = kernel_call(first_half_kernel, half_outputs, output_behind)
    far_outputs = [around(half, 1)]
    (half,) = kernel_call(second_half_kernel, half_outputs, output_ahead)
    far_outputs.append(around(half, -1))
    (branches,) = kernel_call(
        finish_kernel,
        [held((length, 2 * STATE), BF16)],
        lax.axis_index("sp_0").astype(jnp.int32).reshape(1),
        pieces,
        before,
        y,
        reads,
        reach,
        gate,
        pool,
        gated_norm_scale.reshape(1, STATE),
    )
    branches = lax.all_to_all(
        branches.reshape(ring, 2 * own_rows, 2 * STATE), "x", 0, 0, tiled=True
    )
    keep, send = kernel_call(
        output_kernel,
        [held((own_rows, width), F32), held((own_rows, width), BF16)],
        place,
        branches,
        own_output,
        output_behind,
        output_ahead,
        *far_outputs,
        scratch=[pltpu.VMEM((2 * own_rows, width), F32)],
        mebibytes=24,
    )
    (mixed,) = kernel_call(
        join_kernel, [held((own_rows, width), BF16)], keep, swapped(send), mebibytes=8
    )
    return mixed


def solution(mesh):
    ranges = mesh.shape["sp"]
    inner = 8 if ranges % 8 == 0 else 2
    shape = (ranges // inner, inner, mesh.shape["tp"] // 2, 2)
    torus = Mesh(mesh.devices.reshape(shape), SP_TP)
    in_specs = (
        P(SP_TP, None),
        P(),
        P(None, TP),
        P(None, TP),
        P(None, TP),
        P(None, TP),
        P(),
        P(None, TP),
        P(None, TP),
        P(None, TP),
        P(None, TP),
        P(),
        P(TP, SP),
        P(TP, SP),
        P(TP),
        P(TP, None, None),
        P(TP),
        P(TP, None),
        P(TP, None),
    )

    return jax.shard_map(
        shards, mesh=torus, in_specs=in_specs, out_specs=P(SP_TP, None), check_vma=False
    )
```

```python
import jax
import jax.numpy as jnp
from jax import lax
from jax.experimental import pallas as pl
from jax.experimental.pallas import tpu as pltpu
from jax.sharding import Mesh
from jax.sharding import PartitionSpec as P

HEAD_DIM = 64
STATE = 128
BLOCK = 128
POOL_DIM = 64
HALO = 16
SP = ("sp_0", "sp_1")
TP = ("x", "core")
SP_TP = ("sp_0", "sp_1", "x", "core")
EPS = 1e-06
F32 = jnp.float32
BF16 = jnp.bfloat16
STEP_ROWS = 256
PACKED = STATE + 16


def silu(x):
    return x / (1.0 + jnp.exp(-x))


def by_head(first, second, shape):
    lane = lax.broadcasted_iota(jnp.int32, shape, len(shape) - 1)
    return jnp.where(lane < HEAD_DIM, first, second)


def fetch(pairs, arrived):
    copies = [
        pltpu.make_async_copy(source, target, arrived.at[k])
        for k, (source, target) in enumerate(pairs)
    ]
    for copy in copies:
        copy.start()
    for copy in copies:
        copy.wait()


def norm_kernel(x_hbm, scale_hbm, out_ref, tail_ref, x_ref, scale_ref, arrived):
    fetch(((x_hbm, x_ref), (scale_hbm, scale_ref)), arrived)
    rows = normalize(x_ref[...], scale_ref[...])
    out_ref[...] = rows
    tail_ref[...] = rows[rows.shape[0] - HALO :]


def prepare_kernel(
    place_ref,
    value_hbm,
    write_hbm,
    read_hbm,
    pool_hbm,
    gate_hbm,
    *refs,
):
    small_hbm, (w_ref, taps_ref, lanes_ref, pool_matrix_ref), small = (
        refs[:9],
        refs[9:13],
        refs[13:22],
    )
    arrived = refs[22]
    step_ref, value_taps, write_taps, read_taps, bias_ref, pld_ref, rate_ref = small[:7]
    group_ref, channel_ref = small[7:]
    large = [
        (ref, w_ref.at[:, k * STATE : (k + 1) * STATE])
        for k, ref in enumerate((value_hbm, write_hbm, read_hbm, pool_hbm, gate_hbm))
    ]
    fetch(large + list(zip(small_hbm, small)), arrived)
    rank = place_ref[1] * 2 + place_ref[2]
    heads, length = bias_ref.shape
    shape = (step_ref.shape[0], STATE)
    row, lane = (lax.broadcasted_iota(jnp.int32, shape, k) for k in range(2))
    chosen = jnp.where((lane < heads) & (row == rank * heads + lane), 1.0, 0.0).astype(BF16)
    w_ref[:, 5 * STATE :] = lax.dot_general(
        step_ref[...], chosen, (((0,), (0,)), ((), ())), preferred_element_type=F32
    ).astype(BF16)
    for k, ref in enumerate((value_taps, write_taps, read_taps)):
        taps_ref[0:4, k * STATE : (k + 1) * STATE] = ref[...]
    blocks = length // BLOCK
    pairs = heads * blocks
    for b in range(blocks):
        at = slice(b * BLOCK, (b + 1) * BLOCK)
        lanes_ref[b * heads : (b + 1) * heads] = bias_ref[:, at]
        lanes_ref[pairs + b * heads : pairs + (b + 1) * heads] = pld_ref[:, at]
    rates = rate_ref[...]
    at_head = lax.broadcasted_iota(jnp.int32, rates.shape, 1)
    own = [
        jnp.sum(jnp.where(at_head == rank * heads + h, rates, 0.0), axis=1, keepdims=True)
        for h in range(2)
    ]
    odd = lax.broadcasted_iota(jnp.int32, (pairs, BLOCK), 0) % 2 == 1
    lanes_ref[2 * pairs : 3 * pairs] = jnp.exp(jnp.where(odd, own[1], own[0]))
    at_lane = lax.broadcasted_iota(jnp.int32, (1, STATE), 1)
    level = (rank * 2 + at_lane // POOL_DIM) % 4
    window = jnp.where(
        level == 0, 2.0, jnp.where(level == 1, 4.0, jnp.where(level == 2, 8.0, 16.0))
    )
    lanes_ref[3 * pairs : 3 * pairs + 1] = window
    lanes_ref[3 * pairs + 1 : 3 * pairs + 2] = channel_ref[...]
    shape = (POOL_DIM, STATE)
    row, lane = (lax.broadcasted_iota(jnp.int32, shape, k) for k in range(2))
    for k in range(2):
        place = jnp.where(lane == row + k * POOL_DIM, 1.0, 0.0).astype(BF16)
        pool_matrix_ref[k * POOL_DIM : (k + 1) * POOL_DIM] = jnp.dot(
            group_ref[k], place, preferred_element_type=F32
        ).astype(BF16)


def stack_kernel(state_hbm, pool_hbm, out_ref, arrived):
    count = state_hbm.shape[0]
    fetch(((state_hbm, out_ref.at[:count]), (pool_hbm, out_ref.at[count:])), arrived)


def halves_kernel(prior_ref, next_ref, first_ref, second_ref):
    half = first_ref.shape[0]
    first_ref[...] = prior_ref[:half]
    second_ref[...] = next_ref[half:]


def project_kernel(*refs):
    *row_refs, w_ref, other_ref, own_out, other_out, rows_ref = refs
    at = 0
    tails = [ref[...] for ref in row_refs if ref.shape[0] == HALO]
    for ref in row_refs:
        if ref.shape[0] != HALO:
            rows_ref[at : at + ref.shape[0]] = ref[...]
            at += ref.shape[0]
    if tails:
        tail = tails[0]
        for other in tails[1:]:
            tail = tail + other
        rows_ref[at:] = tail
    rows = rows_ref[...]
    own_out[...] = jnp.dot(rows, w_ref[...], preferred_element_type=F32).astype(BF16)
    other_out[...] = jnp.dot(rows, other_ref[...], preferred_element_type=F32).astype(BF16)


def mix_kernel(
    place_ref,
    own_near_ref,
    own_far_ref,
    other_near_ref,
    other_far_ref,
    taps_ref,
    lanes_ref,
    pool_matrix_ref,
    y_ref,
    reads_ref,
    reach_ref,
    gate_ref,
    pool_ref,
    state_ref,
    conv_in,
    pool_in,
    step_in,
    mixed_ref,
):
    length = y_ref.shape[0]
    chunks = length // STEP_ROWS
    blocks = length // BLOCK
    pairs = 2 * blocks
    bias, pld, rate = (lanes_ref[k * pairs : (k + 1) * pairs] for k in range(3))
    window = lanes_ref[3 * pairs : 3 * pairs + 1]
    pool_scale = lanes_ref[3 * pairs + 1 : 3 * pairs + 2]
    base, x, core = place_ref[0], place_ref[1], place_ref[2]
    near = own_near_ref.shape[0] - HALO
    halo = jnp.where(
        core == 0, own_near_ref[near:].astype(F32), other_near_ref[near:].astype(F32)
    )
    conv_in[:HALO] = halo[:, : 3 * STATE]
    pool_in[:HALO] = halo[:, 3 * STATE : 4 * STATE]
    ring = blocks // 2
    for side, near_ref, far_ref in ((core, own_near_ref, own_far_ref), (1 - core, other_near_ref, other_far_ref)):
        for away, source in ((0, near_ref[:BLOCK]), (ring - 1, near_ref[BLOCK : 2 * BLOCK]), (1, near_ref[2 * BLOCK : 3 * BLOCK]), (2, far_ref[...])):
            first = pl.multiple_of(((x + away) % ring * 2 + side) * BLOCK, BLOCK)
            wide = source.astype(F32)
            conv_in[pl.ds(HALO + first, BLOCK)] = wide[:, : 3 * STATE]
            pool_in[pl.ds(HALO + first, BLOCK)] = wide[:, 3 * STATE : 4 * STATE]
            gate_ref[pl.ds(first, BLOCK)] = silu(wide[:, 4 * STATE : 5 * STATE])
            step_in[pl.ds(first, BLOCK)] = wide[:, 5 * STATE :]
    for c in range(chunks):
        first = c * STEP_ROWS
        at = slice(first, first + STEP_ROWS)
        reached = slice(first, first + HALO + STEP_ROWS)
        extended = conv_in[reached]
        summed = extended * taps_ref[3:4, :]
        for back in range(1, 4):
            summed = summed + pltpu.roll(extended, back, 0) * taps_ref[3 - back : 4 - back, :]
        convolved = silu(summed[HALO:]).astype(BF16)
        mixed_ref[at] = convolved[:, : 2 * STATE]
        reads_ref[at] = convolved[:, 2 * STATE :]

        wide = pool_in[reached]
        sum_two = wide + pltpu.roll(wide, 1, 0)
        sum_four = sum_two + pltpu.roll(sum_two, 2, 0)
        sum_eight = sum_four + pltpu.roll(sum_four, 4, 0)
        sum_sixteen = sum_eight + pltpu.roll(sum_eight, 8, 0)
        window_sum = jnp.where(
            window == 2.0,
            sum_two,
            jnp.where(window == 4.0, sum_four, jnp.where(window == 8.0, sum_eight, sum_sixteen)),
        )[HALO:]
        position = (
            base + first + 1 + lax.broadcasted_iota(jnp.int32, (STEP_ROWS, 1), 0)
        ).astype(F32)
        difference = (window_sum / jnp.minimum(position, window) - wide[HALO:]).astype(BF16)
        pooled = jnp.dot(difference, pool_matrix_ref[...], preferred_element_type=F32)
        pool_ref[at] = (pooled * pool_scale).astype(BF16)

    square = (BLOCK, BLOCK)
    row_at = lax.broadcasted_iota(jnp.int32, square, 0)
    col_at = lax.broadcasted_iota(jnp.int32, square, 1)
    upper = (row_at <= col_at).astype(F32)
    causal = row_at >= col_at
    spread = step_in[:BLOCK]
    for b in range(1, blocks):
        spread = spread + pltpu.roll(step_in[b * BLOCK : (b + 1) * BLOCK], 2 * b, 1)
    step = jax.nn.softplus(spread.T[:pairs] + bias)
    cum = jnp.dot(
        pld - rate * step,
        upper,
        precision=lax.Precision.HIGHEST,
        preferred_element_type=F32,
    )
    total = jnp.broadcast_to(cum[:, BLOCK - 1 :], (pairs, BLOCK))
    prefix = jnp.zeros((2, BLOCK), F32)
    prefixes = []
    for b in range(blocks):
        prefixes.append(prefix)
        prefix = prefix + total[2 * b : 2 * b + 2]
    columns = jnp.concatenate(
        [
            cum,
            jnp.exp(total - cum) * step,
            jnp.exp(cum),
            jnp.exp(jnp.concatenate(prefixes, axis=0) + cum),
            jnp.zeros((BLOCK - 4 * pairs, BLOCK), F32),
        ],
        axis=0,
    ).T

    def column(kind, b, h):
        j = kind * pairs + 2 * b + h
        return columns[:, j : j + 1]

    carried = jnp.zeros((STATE, STATE), F32)
    for b in range(blocks):
        at = slice(b * BLOCK, (b + 1) * BLOCK)
        values = mixed_ref[at, :STATE]
        writes = mixed_ref[at, STATE:]
        reads = reads_ref[at]
        affinity = lax.dot_general(
            reads, writes, (((1,), (1,)), ((), ())), preferred_element_type=F32
        )
        inside = []
        for h in range(2):
            row = 2 * b + h
            spacing = column(0, b, h) - cum[row : row + 1]
            within = affinity * jnp.exp(jnp.where(causal, spacing, -jnp.inf)) * step[row : row + 1]
            inside.append(jnp.dot(within.astype(BF16), values, preferred_element_type=F32))
        weighted = (
            values.astype(F32) * by_head(column(1, b, 0), column(1, b, 1), square)
        ).astype(BF16)
        contrib = lax.dot_general(
            writes, weighted, (((0,), (0,)), ((), ())), preferred_element_type=F32
        )
        local = jnp.dot(reads, carried.astype(BF16), preferred_element_type=F32)
        y_ref[at] = by_head(inside[0], inside[1], square) + local * by_head(
            column(2, b, 0), column(2, b, 1), square
        )
        reach_ref[at] = by_head(column(3, b, 0), column(3, b, 1), square)
        decay = by_head(total[2 * b : 2 * b + 1], total[2 * b + 1 : 2 * b + 2], (1, STATE))
        carried = carried * jnp.exp(decay) + contrib
    packed = pack(carried, by_head(prefix[0:1], prefix[1:2], (1, STATE)))
    for k in range(state_ref.shape[0]):
        state_ref[k] = packed


def pack(state, total):
    high = total.astype(BF16)
    low = (total - high.astype(F32)).astype(BF16)
    row = lax.broadcasted_iota(jnp.int32, (PACKED - STATE, STATE), 0)
    tail = jnp.where(row == 0, high.astype(F32), jnp.where(row == 1, low.astype(F32), 0.0))
    return jnp.concatenate([state.astype(BF16), tail.astype(BF16)], axis=0)


def scan_pieces(pieces_ref, here):
    state = before_state = jnp.zeros((STATE, STATE), F32)
    total = before_total = jnp.zeros((1, STATE), F32)
    for k in range(pieces_ref.shape[0]):
        tail = pieces_ref[k, STATE:, :].astype(F32)
        decay = tail[0:1, :] + tail[1:2, :]
        state = state * jnp.exp(decay) + pieces_ref[k, :STATE, :].astype(F32)
        total = total + decay
        passed = k < here
        before_state = jnp.where(passed, state, before_state)
        before_total = jnp.where(passed, total, before_total)
    return state, total, before_state, before_total


def row_scan_kernel(here_ref, pieces_ref, before_ref, packed_ref):
    state, total, before_state, before_total = scan_pieces(pieces_ref, here_ref[0])
    before_ref[:STATE, :] = before_state
    before_ref[STATE:, :] = jnp.broadcast_to(before_total, (8, STATE))
    packed = pack(state, total)
    for k in range(packed_ref.shape[0]):
        packed_ref[k] = packed


def finish_kernel(
    here_ref,
    pieces_ref,
    before_ref,
    y_ref,
    reads_ref,
    reach_ref,
    gate_ref,
    pool_ref,
    scale_ref,
    out_ref,
):
    _, _, rows_before, _ = scan_pieces(pieces_ref, here_ref[0])
    incoming = rows_before * jnp.exp(before_ref[STATE : STATE + 1, :]) + before_ref[:STATE, :]
    crossed = jnp.dot(reads_ref[...], incoming.astype(BF16), preferred_element_type=F32)
    gated = (y_ref[...] + crossed * reach_ref[...]) * gate_ref[...]
    norm = lax.rsqrt(jnp.mean(gated * gated, axis=-1, keepdims=True) + EPS)
    out_ref[:, :STATE] = (gated * norm * scale_ref[...]).astype(BF16)
    out_ref[:, STATE:] = pool_ref[...]


def output_kernel(rows_ref, w_ref, out_ref, weights_ref, arrived):
    parts = rows_ref.shape[0]
    incoming = [
        pltpu.make_async_copy(w_ref.at[k], weights_ref.at[k], arrived.at[k]) for k in range(parts)
    ]
    for copy in incoming[:3]:
        copy.start()
    total = None
    for k in range(parts):
        incoming[k].wait()
        if k + 3 < parts:
            incoming[k + 3].start()
        part = jnp.dot(rows_ref[k], weights_ref[k], preferred_element_type=F32)
        total = part if total is None else total + part
    out_ref[...] = total.astype(BF16)


def limits(mebibytes):
    return pltpu.CompilerParams(vmem_limit_bytes=mebibytes * 2**20)


def whole(shape):
    return pl.BlockSpec(shape, lambda *_: (0,) * len(shape))


def normalize(rows, scale):
    wide = rows.astype(F32)
    return (wide * lax.rsqrt(jnp.mean(wide * wide, axis=-1, keepdims=True) + EPS) * scale).astype(
        BF16
    )


def rows_before(rows, ring):
    ranges = lax.axis_size(SP)
    members = 2 * ring
    return [
        lax.ppermute(
            rows,
            SP_TP,
            [(i * members + members - 1, (i + 1) * members + 2 * k) for i in range(ranges - 1)],
        )
        for k in range(ring)
    ]


def around(array, away):
    ring = lax.axis_size("x")
    return lax.ppermute(array, "x", [(i, (i + away) % ring) for i in range(ring)])


def swapped(array):
    return lax.ppermute(array, "core", [(0, 1), (1, 0)])


class Stored:
    def __init__(self, array):
        self.array = pltpu.with_memory_space_constraint(array, pltpu.HBM)
        self.shape, self.dtype = array.shape, array.dtype


def kernel_call(body, out_shape, *arrays, scratch=(), mebibytes=16):
    def spec(array):
        if isinstance(array, Stored):
            return pl.BlockSpec(memory_space=pltpu.HBM)
        if array.ndim == 1:
            return pl.BlockSpec(memory_space=pltpu.SMEM)
        return whole(array.shape)

    return pl.pallas_call(
        body,
        grid=(1,),
        in_specs=[spec(array) for array in arrays],
        out_specs=[whole(out.shape) for out in out_shape],
        out_shape=out_shape,
        scratch_shapes=list(scratch),
        compiler_params=limits(mebibytes),
    )(*(array.array if isinstance(array, Stored) else array for array in arrays))


def held(shape, dtype):
    return jax.ShapeDtypeStruct(shape, dtype)


def shards(
    activations,
    input_norm_scale,
    value_weight_matrix,
    gate_weight_matrix,
    write_weight_matrix,
    read_weight_matrix,
    step_weight_matrix,
    pooling_input_matrix,
    value_filter_weight,
    write_filter_weight,
    read_filter_weight,
    head_log_decay_rate,
    step_bias_offset,
    position_log_decay,
    gated_norm_scale,
    pooling_group_matrix,
    pooling_channel_scale,
    state_output_matrix,
    pooling_output_matrix,
):
    x, core = lax.axis_index("x"), lax.axis_index("core")
    ring = lax.axis_size("x")
    sp_rank = lax.axis_index(SP)
    own_rows, width = activations.shape
    length = own_rows * ring * 2
    blocks = length // BLOCK
    scale = input_norm_scale.reshape(1, width)

    place = jnp.stack([sp_rank * length, x, core]).astype(jnp.int32)
    normed, tail = kernel_call(
        norm_kernel,
        [held((own_rows, width), BF16), held((HALO, width), BF16)],
        Stored(activations),
        Stored(scale),
        scratch=[
            pltpu.VMEM((own_rows, width), BF16),
            pltpu.VMEM((1, width), F32),
            pltpu.SemaphoreType.DMA((2,)),
        ],
    )
    prior = around(normed, 1)
    following = around(normed, -1)
    found = rows_before(tail, ring)
    output_rows = state_output_matrix.shape[0] + pooling_output_matrix.shape[0]
    (own_output,) = kernel_call(
        stack_kernel,
        [held((output_rows, width), BF16)],
        Stored(state_output_matrix),
        Stored(pooling_output_matrix),
        scratch=[pltpu.SemaphoreType.DMA((2,))],
    )
    output_weights = lax.all_gather(own_output, TP, axis=0)
    small = [
        step_weight_matrix.T,
        value_filter_weight,
        write_filter_weight,
        read_filter_weight,
        step_bias_offset,
        position_log_decay,
        head_log_decay_rate.reshape(1, -1),
        pooling_group_matrix,
        pooling_channel_scale.reshape(1, STATE),
    ]
    large = [
        value_weight_matrix,
        write_weight_matrix,
        read_weight_matrix,
        pooling_input_matrix,
        gate_weight_matrix,
    ]
    weights, taps, lanes, pool_matrix = kernel_call(
        prepare_kernel,
        [
            held((width, 6 * STATE), BF16),
            held((8, 3 * STATE), F32),
            held((6 * blocks + 8, STATE), F32),
            held((STATE, STATE), BF16),
        ],
        place,
        *(Stored(array) for array in large + small),
        scratch=[pltpu.VMEM(array.shape, array.dtype) for array in small]
        + [pltpu.SemaphoreType.DMA((len(large) + len(small),))],
    )
    other_weights = swapped(weights)
    half = own_rows // 2
    far = kernel_call(halves_kernel, [held((half, width), BF16)] * 2, prior, following)
    far_first = around(far[0], 1)
    far_second = around(far[1], -1)

    def project(*pieces):
        count = sum(piece.shape[0] for piece in pieces if piece.shape[0] > HALO)
        count += HALO * any(piece.shape[0] == HALO for piece in pieces)
        return kernel_call(
            project_kernel,
            [held((count, weights.shape[1]), BF16)] * 2,
            *pieces,
            weights,
            other_weights,
            scratch=[pltpu.VMEM((count, width), BF16)],
            mebibytes=24,
        )

    own_near, send_near = project(normed, prior, following, *found)
    other_near = swapped(send_near)
    own_far, send_far = project(far_first, far_second)
    other_far = swapped(send_far)

    columns, inner = lax.axis_size("sp_0"), lax.axis_size("sp_1")
    y, reads, reach, gate, pool, packed = kernel_call(
        mix_kernel,
        [
            held((length, STATE), F32),
            held((length, STATE), BF16),
            held((length, STATE), F32),
            held((length, STATE), F32),
            held((length, STATE), BF16),
            held((inner, PACKED, STATE), BF16),
        ],
        place,
        own_near,
        own_far,
        other_near,
        other_far,
        taps,
        lanes,
        pool_matrix,
        scratch=[
            pltpu.VMEM((HALO + length, 3 * STATE), F32),
            pltpu.VMEM((HALO + length, STATE), F32),
            pltpu.VMEM((length, STATE), F32),
            pltpu.VMEM((length, 2 * STATE), BF16),
        ],
        mebibytes=24,
    )

    pieces = lax.all_to_all(packed, "sp_1", 0, 0, tiled=True)
    before, packed = kernel_call(
        row_scan_kernel,
        [held((STATE + 8, STATE), F32), held((columns, PACKED, STATE), BF16)],
        lax.axis_index("sp_1").astype(jnp.int32).reshape(1),
        pieces,
        mebibytes=8,
    )
    pieces = lax.all_to_all(packed, "sp_0", 0, 0, tiled=True)
    (branches,) = kernel_call(
        finish_kernel,
        [held((length, 2 * STATE), BF16)],
        lax.axis_index("sp_0").astype(jnp.int32).reshape(1),
        pieces,
        before,
        y,
        reads,
        reach,
        gate,
        pool,
        gated_norm_scale.reshape(1, STATE),
    )
    members = 2 * ring
    branches = lax.all_to_all(
        branches.reshape(members, own_rows, 2 * STATE), TP, 0, 0, tiled=True
    )
    (mixed,) = kernel_call(
        output_kernel,
        [held((own_rows, width), BF16)],
        branches,
        Stored(output_weights),
        scratch=[
            pltpu.VMEM((members, 2 * STATE, width), BF16),
            pltpu.SemaphoreType.DMA((members,)),
        ],
        mebibytes=20,
    )
    return mixed


def solution(mesh):
    ranges = mesh.shape["sp"]
    inner = 8 if ranges % 8 == 0 else 2
    shape = (ranges // inner, inner, mesh.shape["tp"] // 2, 2)
    torus = Mesh(mesh.devices.reshape(shape), SP_TP)
    in_specs = (
        P(SP_TP, None),
        P(),
        P(None, TP),
        P(None, TP),
        P(None, TP),
        P(None, TP),
        P(),
        P(None, TP),
        P(None, TP),
        P(None, TP),
        P(None, TP),
        P(),
        P(TP, SP),
        P(TP, SP),
        P(TP),
        P(TP, None, None),
        P(TP),
        P(TP, None),
        P(TP, None),
    )

    return jax.shard_map(
        shards, mesh=torus, in_specs=in_specs, out_specs=P(SP_TP, None), check_vma=False
    )
```

```python
import jax
import jax.numpy as jnp
from jax import lax
from jax.experimental import pallas as pl
from jax.experimental.pallas import tpu as pltpu
from jax.sharding import Mesh
from jax.sharding import PartitionSpec as P

HEAD_DIM = 64
STATE = 128
BLOCK = 128
POOL_DIM = 64
HALO = 16
SP = ("sp_0", "sp_1")
TP = ("x", "core")
SP_TP = ("sp_0", "sp_1", "x", "core")
EPS = 1e-06
F32 = jnp.float32
BF16 = jnp.bfloat16
STEP_ROWS = 256
PACKED = STATE + 16


def silu(x):
    return x / (1.0 + jnp.exp(-x))


def by_head(first, second, shape):
    lane = lax.broadcasted_iota(jnp.int32, shape, len(shape) - 1)
    return jnp.where(lane < HEAD_DIM, first, second)


def fetch(pairs, arrived):
    copies = [
        pltpu.make_async_copy(source, target, arrived.at[k])
        for k, (source, target) in enumerate(pairs)
    ]
    for copy in copies:
        copy.start()
    for copy in copies:
        copy.wait()


def norm_kernel(x_hbm, scale_hbm, out_ref, tail_ref, x_ref, scale_ref, arrived):
    fetch(((x_hbm, x_ref), (scale_hbm, scale_ref)), arrived)
    rows = normalize(x_ref[...], scale_ref[...])
    out_ref[...] = rows
    tail_ref[...] = rows[rows.shape[0] - HALO :]


def prepare_kernel(
    place_ref,
    value_hbm,
    write_hbm,
    read_hbm,
    pool_hbm,
    gate_hbm,
    state_output_hbm,
    pool_output_hbm,
    *refs,
):
    small_hbm, (w_ref, output_ref, taps_ref, lanes_ref, pool_matrix_ref), small = (
        refs[:9],
        refs[9:14],
        refs[14:23],
    )
    arrived = refs[23]
    step_ref, value_taps, write_taps, read_taps, bias_ref, pld_ref, rate_ref = small[:7]
    group_ref, channel_ref = small[7:]
    count = state_output_hbm.shape[0]
    large = [
        (ref, w_ref.at[:, k * STATE : (k + 1) * STATE])
        for k, ref in enumerate((value_hbm, write_hbm, read_hbm, pool_hbm, gate_hbm))
    ]
    large.append((state_output_hbm, output_ref.at[:count]))
    large.append((pool_output_hbm, output_ref.at[count:]))
    fetch(large + list(zip(small_hbm, small)), arrived)
    rank = place_ref[1] * 2 + place_ref[2]
    heads, length = bias_ref.shape
    shape = (step_ref.shape[0], STATE)
    row, lane = (lax.broadcasted_iota(jnp.int32, shape, k) for k in range(2))
    chosen = jnp.where((lane < heads) & (row == rank * heads + lane), 1.0, 0.0).astype(BF16)
    w_ref[:, 5 * STATE :] = lax.dot_general(
        step_ref[...], chosen, (((0,), (0,)), ((), ())), preferred_element_type=F32
    ).astype(BF16)
    for k, ref in enumerate((value_taps, write_taps, read_taps)):
        taps_ref[0:4, k * STATE : (k + 1) * STATE] = ref[...]
    blocks = length // BLOCK
    pairs = heads * blocks
    for b in range(blocks):
        at = slice(b * BLOCK, (b + 1) * BLOCK)
        lanes_ref[b * heads : (b + 1) * heads] = bias_ref[:, at]
        lanes_ref[pairs + b * heads : pairs + (b + 1) * heads] = pld_ref[:, at]
    rates = rate_ref[...]
    at_head = lax.broadcasted_iota(jnp.int32, rates.shape, 1)
    own = [
        jnp.sum(jnp.where(at_head == rank * heads + h, rates, 0.0), axis=1, keepdims=True)
        for h in range(2)
    ]
    odd = lax.broadcasted_iota(jnp.int32, (pairs, BLOCK), 0) % 2 == 1
    lanes_ref[2 * pairs : 3 * pairs] = jnp.exp(jnp.where(odd, own[1], own[0]))
    at_lane = lax.broadcasted_iota(jnp.int32, (1, STATE), 1)
    level = (rank * 2 + at_lane // POOL_DIM) % 4
    window = jnp.where(
        level == 0, 2.0, jnp.where(level == 1, 4.0, jnp.where(level == 2, 8.0, 16.0))
    )
    lanes_ref[3 * pairs : 3 * pairs + 1] = window
    lanes_ref[3 * pairs + 1 : 3 * pairs + 2] = channel_ref[...]
    shape = (POOL_DIM, STATE)
    row, lane = (lax.broadcasted_iota(jnp.int32, shape, k) for k in range(2))
    for k in range(2):
        place = jnp.where(lane == row + k * POOL_DIM, 1.0, 0.0).astype(BF16)
        pool_matrix_ref[k * POOL_DIM : (k + 1) * POOL_DIM] = jnp.dot(
            group_ref[k], place, preferred_element_type=F32
        ).astype(BF16)


def halves_kernel(prior_ref, next_ref, first_ref, second_ref):
    half = first_ref.shape[0]
    first_ref[...] = prior_ref[:half]
    second_ref[...] = next_ref[half:]


def project_kernel(*refs):
    *row_refs, w_ref, other_hbm, own_out, other_out, rows_ref, other_ref, arrived = refs
    copy = pltpu.make_async_copy(other_hbm, other_ref, arrived)
    copy.start()
    at = 0
    tails = [ref[...] for ref in row_refs if ref.shape[0] == HALO]
    for ref in row_refs:
        if ref.shape[0] != HALO:
            rows_ref[at : at + ref.shape[0]] = ref[...]
            at += ref.shape[0]
    if tails:
        tail = tails[0]
        for other in tails[1:]:
            tail = tail + other
        rows_ref[at:] = tail
    rows = rows_ref[...]
    own_out[...] = jnp.dot(rows, w_ref[...], preferred_element_type=F32).astype(BF16)
    copy.wait()
    other_out[...] = jnp.dot(rows, other_ref[...], preferred_element_type=F32).astype(BF16)


def mix_kernel(
    place_ref,
    own_near_ref,
    own_far_ref,
    other_near_ref,
    other_far_ref,
    taps_ref,
    lanes_ref,
    pool_matrix_ref,
    y_ref,
    reads_ref,
    reach_ref,
    gate_ref,
    pool_ref,
    state_ref,
    conv_in,
    pool_in,
    step_in,
    mixed_ref,
):
    length = y_ref.shape[0]
    chunks = length // STEP_ROWS
    blocks = length // BLOCK
    pairs = 2 * blocks
    bias, pld, rate = (lanes_ref[k * pairs : (k + 1) * pairs] for k in range(3))
    window = lanes_ref[3 * pairs : 3 * pairs + 1]
    pool_scale = lanes_ref[3 * pairs + 1 : 3 * pairs + 2]
    base, x, core = place_ref[0], place_ref[1], place_ref[2]
    near = own_near_ref.shape[0] - HALO
    halo = jnp.where(
        core == 0, own_near_ref[near:].astype(F32), other_near_ref[near:].astype(F32)
    )
    conv_in[:HALO] = halo[:, : 3 * STATE]
    pool_in[:HALO] = halo[:, 3 * STATE : 4 * STATE]
    ring = blocks // 2
    for side, near_ref, far_ref in ((core, own_near_ref, own_far_ref), (1 - core, other_near_ref, other_far_ref)):
        for away, source in ((0, near_ref[:BLOCK]), (ring - 1, near_ref[BLOCK : 2 * BLOCK]), (1, near_ref[2 * BLOCK : 3 * BLOCK]), (2, far_ref[...])):
            first = pl.multiple_of(((x + away) % ring * 2 + side) * BLOCK, BLOCK)
            wide = source.astype(F32)
            conv_in[pl.ds(HALO + first, BLOCK)] = wide[:, : 3 * STATE]
            pool_in[pl.ds(HALO + first, BLOCK)] = wide[:, 3 * STATE : 4 * STATE]
            gate_ref[pl.ds(first, BLOCK)] = silu(wide[:, 4 * STATE : 5 * STATE])
            step_in[pl.ds(first, BLOCK)] = wide[:, 5 * STATE :]
    for c in range(chunks):
        first = c * STEP_ROWS
        at = slice(first, first + STEP_ROWS)
        reached = slice(first, first + HALO + STEP_ROWS)
        extended = conv_in[reached]
        summed = extended * taps_ref[3:4, :]
        for back in range(1, 4):
            summed = summed + pltpu.roll(extended, back, 0) * taps_ref[3 - back : 4 - back, :]
        convolved = silu(summed[HALO:]).astype(BF16)
        mixed_ref[at] = convolved[:, : 2 * STATE]
        reads_ref[at] = convolved[:, 2 * STATE :]

        wide = pool_in[reached]
        sum_two = wide + pltpu.roll(wide, 1, 0)
        sum_four = sum_two + pltpu.roll(sum_two, 2, 0)
        sum_eight = sum_four + pltpu.roll(sum_four, 4, 0)
        sum_sixteen = sum_eight + pltpu.roll(sum_eight, 8, 0)
        window_sum = jnp.where(
            window == 2.0,
            sum_two,
            jnp.where(window == 4.0, sum_four, jnp.where(window == 8.0, sum_eight, sum_sixteen)),
        )[HALO:]
        position = (
            base + first + 1 + lax.broadcasted_iota(jnp.int32, (STEP_ROWS, 1), 0)
        ).astype(F32)
        difference = (window_sum / jnp.minimum(position, window) - wide[HALO:]).astype(BF16)
        pooled = jnp.dot(difference, pool_matrix_ref[...], preferred_element_type=F32)
        pool_ref[at] = (pooled * pool_scale).astype(BF16)

    square = (BLOCK, BLOCK)
    row_at = lax.broadcasted_iota(jnp.int32, square, 0)
    col_at = lax.broadcasted_iota(jnp.int32, square, 1)
    upper = (row_at <= col_at).astype(F32)
    causal = row_at >= col_at
    spread = step_in[:BLOCK]
    for b in range(1, blocks):
        spread = spread + pltpu.roll(step_in[b * BLOCK : (b + 1) * BLOCK], 2 * b, 1)
    step = jax.nn.softplus(spread.T[:pairs] + bias)
    cum = jnp.dot(
        pld - rate * step,
        upper,
        precision=lax.Precision.HIGHEST,
        preferred_element_type=F32,
    )
    total = jnp.broadcast_to(cum[:, BLOCK - 1 :], (pairs, BLOCK))
    prefix = jnp.zeros((2, BLOCK), F32)
    prefixes = []
    for b in range(blocks):
        prefixes.append(prefix)
        prefix = prefix + total[2 * b : 2 * b + 2]
    columns = jnp.concatenate(
        [
            cum,
            jnp.exp(total - cum) * step,
            jnp.exp(cum),
            jnp.exp(jnp.concatenate(prefixes, axis=0) + cum),
            jnp.zeros((BLOCK - 4 * pairs, BLOCK), F32),
        ],
        axis=0,
    ).T

    def column(kind, b, h):
        j = kind * pairs + 2 * b + h
        return columns[:, j : j + 1]

    carried = jnp.zeros((STATE, STATE), F32)
    for b in range(blocks):
        at = slice(b * BLOCK, (b + 1) * BLOCK)
        values = mixed_ref[at, :STATE]
        writes = mixed_ref[at, STATE:]
        reads = reads_ref[at]
        affinity = lax.dot_general(
            reads, writes, (((1,), (1,)), ((), ())), preferred_element_type=F32
        )
        inside = []
        for h in range(2):
            row = 2 * b + h
            spacing = column(0, b, h) - cum[row : row + 1]
            within = affinity * jnp.exp(jnp.where(causal, spacing, -jnp.inf)) * step[row : row + 1]
            inside.append(jnp.dot(within.astype(BF16), values, preferred_element_type=F32))
        weighted = (
            values.astype(F32) * by_head(column(1, b, 0), column(1, b, 1), square)
        ).astype(BF16)
        contrib = lax.dot_general(
            writes, weighted, (((0,), (0,)), ((), ())), preferred_element_type=F32
        )
        local = jnp.dot(reads, carried.astype(BF16), preferred_element_type=F32)
        y_ref[at] = by_head(inside[0], inside[1], square) + local * by_head(
            column(2, b, 0), column(2, b, 1), square
        )
        reach_ref[at] = by_head(column(3, b, 0), column(3, b, 1), square)
        decay = by_head(total[2 * b : 2 * b + 1], total[2 * b + 1 : 2 * b + 2], (1, STATE))
        carried = carried * jnp.exp(decay) + contrib
    packed = pack(carried, by_head(prefix[0:1], prefix[1:2], (1, STATE)))
    for k in range(state_ref.shape[0]):
        state_ref[k] = packed


def pack(state, total):
    high = total.astype(BF16)
    low = (total - high.astype(F32)).astype(BF16)
    row = lax.broadcasted_iota(jnp.int32, (PACKED - STATE, STATE), 0)
    tail = jnp.where(row == 0, high.astype(F32), jnp.where(row == 1, low.astype(F32), 0.0))
    return jnp.concatenate([state.astype(BF16), tail.astype(BF16)], axis=0)


def scan_pieces(pieces_ref, here):
    state = before_state = jnp.zeros((STATE, STATE), F32)
    total = before_total = jnp.zeros((1, STATE), F32)
    for k in range(pieces_ref.shape[0]):
        tail = pieces_ref[k, STATE:, :].astype(F32)
        decay = tail[0:1, :] + tail[1:2, :]
        state = state * jnp.exp(decay) + pieces_ref[k, :STATE, :].astype(F32)
        total = total + decay
        passed = k < here
        before_state = jnp.where(passed, state, before_state)
        before_total = jnp.where(passed, total, before_total)
    return state, total, before_state, before_total


def row_scan_kernel(here_ref, pieces_ref, before_ref, packed_ref):
    state, total, before_state, before_total = scan_pieces(pieces_ref, here_ref[0])
    before_ref[:STATE, :] = before_state
    before_ref[STATE:, :] = jnp.broadcast_to(before_total, (8, STATE))
    packed = pack(state, total)
    for k in range(packed_ref.shape[0]):
        packed_ref[k] = packed


def finish_kernel(
    here_ref,
    pieces_ref,
    before_ref,
    y_ref,
    reads_ref,
    reach_ref,
    gate_ref,
    pool_ref,
    scale_ref,
    out_ref,
):
    _, _, rows_before, _ = scan_pieces(pieces_ref, here_ref[0])
    incoming = rows_before * jnp.exp(before_ref[STATE : STATE + 1, :]) + before_ref[:STATE, :]
    crossed = jnp.dot(reads_ref[...], incoming.astype(BF16), preferred_element_type=F32)
    gated = (y_ref[...] + crossed * reach_ref[...]) * gate_ref[...]
    norm = lax.rsqrt(jnp.mean(gated * gated, axis=-1, keepdims=True) + EPS)
    out_ref[:, :STATE] = (gated * norm * scale_ref[...]).astype(BF16)
    out_ref[:, STATE:] = pool_ref[...]


def output_kernel(rows_ref, w_ref, out_ref, weights_ref, arrived):
    parts = rows_ref.shape[0]
    incoming = [
        pltpu.make_async_copy(w_ref.at[k], weights_ref.at[k], arrived.at[k]) for k in range(parts)
    ]
    for copy in incoming:
        copy.start()
    total = None
    for k in range(parts):
        incoming[k].wait()
        part = jnp.dot(rows_ref[k], weights_ref[k], preferred_element_type=F32)
        total = part if total is None else total + part
    out_ref[...] = total.astype(BF16)


def limits(mebibytes):
    return pltpu.CompilerParams(vmem_limit_bytes=mebibytes * 2**20)


def whole(shape):
    return pl.BlockSpec(shape, lambda *_: (0,) * len(shape))


def normalize(rows, scale):
    wide = rows.astype(F32)
    return (wide * lax.rsqrt(jnp.mean(wide * wide, axis=-1, keepdims=True) + EPS) * scale).astype(
        BF16
    )


def rows_before(rows, ring):
    ranges = lax.axis_size(SP)
    members = 2 * ring
    return [
        lax.ppermute(
            rows,
            SP_TP,
            [(i * members + members - 1, (i + 1) * members + 2 * k) for i in range(ranges - 1)],
        )
        for k in range(ring)
    ]


def around(array, away):
    ring = lax.axis_size("x")
    return lax.ppermute(array, "x", [(i, (i + away) % ring) for i in range(ring)])


def swapped(array):
    return lax.ppermute(array, "core", [(0, 1), (1, 0)])


class Stored:
    def __init__(self, array):
        self.array = pltpu.with_memory_space_constraint(array, pltpu.HBM)
        self.shape, self.dtype = array.shape, array.dtype


def kernel_call(body, out_shape, *arrays, scratch=(), mebibytes=16):
    def spec(array):
        if isinstance(array, Stored):
            return pl.BlockSpec(memory_space=pltpu.HBM)
        if array.ndim == 1:
            return pl.BlockSpec(memory_space=pltpu.SMEM)
        return whole(array.shape)

    return pl.pallas_call(
        body,
        grid=(1,),
        in_specs=[spec(array) for array in arrays],
        out_specs=[whole(out.shape) for out in out_shape],
        out_shape=out_shape,
        scratch_shapes=list(scratch),
        compiler_params=limits(mebibytes),
    )(*(array.array if isinstance(array, Stored) else array for array in arrays))


def held(shape, dtype):
    return jax.ShapeDtypeStruct(shape, dtype)


def shards(
    activations,
    input_norm_scale,
    value_weight_matrix,
    gate_weight_matrix,
    write_weight_matrix,
    read_weight_matrix,
    step_weight_matrix,
    pooling_input_matrix,
    value_filter_weight,
    write_filter_weight,
    read_filter_weight,
    head_log_decay_rate,
    step_bias_offset,
    position_log_decay,
    gated_norm_scale,
    pooling_group_matrix,
    pooling_channel_scale,
    state_output_matrix,
    pooling_output_matrix,
):
    x, core = lax.axis_index("x"), lax.axis_index("core")
    ring = lax.axis_size("x")
    sp_rank = lax.axis_index(SP)
    own_rows, width = activations.shape
    length = own_rows * ring * 2
    blocks = length // BLOCK
    scale = input_norm_scale.reshape(1, width)

    place = jnp.stack([sp_rank * length, x, core]).astype(jnp.int32)
    normed, tail = kernel_call(
        norm_kernel,
        [held((own_rows, width), BF16), held((HALO, width), BF16)],
        Stored(activations),
        Stored(scale),
        scratch=[
            pltpu.VMEM((own_rows, width), BF16),
            pltpu.VMEM((1, width), F32),
            pltpu.SemaphoreType.DMA((2,)),
        ],
    )
    prior = around(normed, 1)
    following = around(normed, -1)
    found = rows_before(tail, ring)
    output_rows = state_output_matrix.shape[0] + pooling_output_matrix.shape[0]
    small = [
        step_weight_matrix.T,
        value_filter_weight,
        write_filter_weight,
        read_filter_weight,
        step_bias_offset,
        position_log_decay,
        head_log_decay_rate.reshape(1, -1),
        pooling_group_matrix,
        pooling_channel_scale.reshape(1, STATE),
    ]
    large = [
        value_weight_matrix,
        write_weight_matrix,
        read_weight_matrix,
        pooling_input_matrix,
        gate_weight_matrix,
        state_output_matrix,
        pooling_output_matrix,
    ]
    weights, own_output, taps, lanes, pool_matrix = kernel_call(
        prepare_kernel,
        [
            held((width, 6 * STATE), BF16),
            held((output_rows, width), BF16),
            held((8, 3 * STATE), F32),
            held((6 * blocks + 8, STATE), F32),
            held((STATE, STATE), BF16),
        ],
        place,
        *(Stored(array) for array in large + small),
        scratch=[pltpu.VMEM(array.shape, array.dtype) for array in small]
        + [pltpu.SemaphoreType.DMA((len(large) + len(small),))],
    )
    other_weights = swapped(weights)
    half = own_rows // 2
    far = kernel_call(halves_kernel, [held((half, width), BF16)] * 2, prior, following)
    far, own_output = lax.optimization_barrier((far, own_output))
    output_weights = lax.all_gather(own_output, TP, axis=0)
    far_first = around(far[0], 1)
    far_second = around(far[1], -1)

    def project(*pieces):
        count = sum(piece.shape[0] for piece in pieces if piece.shape[0] > HALO)
        count += HALO * any(piece.shape[0] == HALO for piece in pieces)
        return kernel_call(
            project_kernel,
            [held((count, weights.shape[1]), BF16)] * 2,
            *pieces,
            weights,
            Stored(other_weights),
            scratch=[
                pltpu.VMEM((count, width), BF16),
                pltpu.VMEM(weights.shape, BF16),
                pltpu.SemaphoreType.DMA,
            ],
            mebibytes=24,
        )

    own_near, send_near = project(normed, prior, following, *found)
    other_near = swapped(send_near)
    own_far, send_far = project(far_first, far_second)
    other_far = swapped(send_far)

    columns, inner = lax.axis_size("sp_0"), lax.axis_size("sp_1")
    y, reads, reach, gate, pool, packed = kernel_call(
        mix_kernel,
        [
            held((length, STATE), F32),
            held((length, STATE), BF16),
            held((length, STATE), F32),
            held((length, STATE), F32),
            held((length, STATE), BF16),
            held((inner, PACKED, STATE), BF16),
        ],
        place,
        own_near,
        own_far,
        other_near,
        other_far,
        taps,
        lanes,
        pool_matrix,
        scratch=[
            pltpu.VMEM((HALO + length, 3 * STATE), F32),
            pltpu.VMEM((HALO + length, STATE), F32),
            pltpu.VMEM((length, STATE), F32),
            pltpu.VMEM((length, 2 * STATE), BF16),
        ],
        mebibytes=24,
    )

    pieces = lax.all_to_all(packed, "sp_1", 0, 0, tiled=True)
    before, packed = kernel_call(
        row_scan_kernel,
        [held((STATE + 8, STATE), F32), held((columns, PACKED, STATE), BF16)],
        lax.axis_index("sp_1").astype(jnp.int32).reshape(1),
        pieces,
        mebibytes=8,
    )
    pieces = lax.all_to_all(packed, "sp_0", 0, 0, tiled=True)
    (branches,) = kernel_call(
        finish_kernel,
        [held((length, 2 * STATE), BF16)],
        lax.axis_index("sp_0").astype(jnp.int32).reshape(1),
        pieces,
        before,
        y,
        reads,
        reach,
        gate,
        pool,
        gated_norm_scale.reshape(1, STATE),
    )
    members = 2 * ring
    branches = lax.all_to_all(
        branches.reshape(members, own_rows, 2 * STATE), TP, 0, 0, tiled=True
    )
    (mixed,) = kernel_call(
        output_kernel,
        [held((own_rows, width), BF16)],
        branches,
        Stored(output_weights),
        scratch=[
            pltpu.VMEM((members, 2 * STATE, width), BF16),
            pltpu.SemaphoreType.DMA((members,)),
        ],
        mebibytes=20,
    )
    return mixed


def solution(mesh):
    ranges = mesh.shape["sp"]
    inner = 8 if ranges % 8 == 0 else 2
    shape = (ranges // inner, inner, mesh.shape["tp"] // 2, 2)
    torus = Mesh(mesh.devices.reshape(shape), SP_TP)
    in_specs = (
        P(SP_TP, None),
        P(),
        P(None, TP),
        P(None, TP),
        P(None, TP),
        P(None, TP),
        P(),
        P(None, TP),
        P(None, TP),
        P(None, TP),
        P(None, TP),
        P(),
        P(TP, SP),
        P(TP, SP),
        P(TP),
        P(TP, None, None),
        P(TP),
        P(TP, None),
        P(TP, None),
    )

    return jax.shard_map(
        shards, mesh=torus, in_specs=in_specs, out_specs=P(SP_TP, None), check_vma=False
    )
```
